32 devices in a mesh: ep: 16 (over z, y, x), tp: 2 (over core).
Axes of the slice: x: 2, y: 2, z: 4, core: 2. Of those that a mesh axis runs over, the one named last changes fastest.
Arguments:
- tokens: bfloat16 [4096, 4096], P('ep'), may hold values from -6 to 6
- cotangent: bfloat16 [4096, 4096], P('ep'), may hold values from -1.5 to 1.5
- gates: float32 [4096, 2], P('ep'), may hold values from 0.05 to 0.95
- experts: int32 [4096, 2], P('ep'), may hold values from 0 to 15, all different within a row; in each aligned block of 256 rows (0 to 255, 256 to 511, ...) at most 48 rows name the same one
- gate_w: bfloat16 [16, 4096, 768], P('ep', None, 'tp'), may hold values from -0.09375 to 0.09375
- up_w: bfloat16 [16, 4096, 768], P('ep', None, 'tp'), may hold values from -0.09375 to 0.09375
- down_w: bfloat16 [16, 768, 4096], P('ep', 'tp'), may hold values from -0.21875 to 0.21875
Outputs:
- grad_tokens: bfloat16 [4096, 4096], P('ep', 'tp')
- grad_gates: float32 [4096, 2], P('ep')
- grad_gate_w: bfloat16 [16, 4096, 768], P('ep', None, 'tp')
- grad_up_w: bfloat16 [16, 4096, 768], P('ep', None, 'tp')
- grad_down_w: bfloat16 [16, 768, 4096], P('ep', 'tp')
- sq_gate: float32 [16, 4096], P('ep')
- sq_up: float32 [16, 4096], P('ep')
- sq_down: float32 [16, 768], P('ep', 'tp')
The draws below stay inside these ranges and needn't reach their ends.
Inputs may be any that keep to these rules, and one draw needn't show every extreme that they name: In each aligned block of 256 rows no expert is named by more than 48 rows, a bound that some expert reaches in some blocks; the 2 experts of a row differ.
All inputs are finite; a program needn't handle non-finite values.
Results may differ from the reference program's by a relative error of at most 0.024.
Values may be sent and summed in bfloat16 or wider, within the bound.
A program may use at most 192 MiB of HBM per device.

```python
import math
import jax
import jax.numpy as jnp
import numpy as np
from jax import lax

D = 4096
FF = 768
TOPK = 2
TOK_DEV = 256
EXPERTS = 16
CAP = 48
TOKENS = 4096
N_EP = 16
N_TP = 2


def level_of(key, dims, shards, low, top_value):
    factor_of, own = 1.0, jax.random.fold_in(key, 6)
    for position, shards_of in shards:
        heights = jnp.exp(jax.random.uniform(jax.random.fold_in(own, position), (shards_of,), jnp.float32, low / len(shards), top_value / len(shards)))
        factor_of = factor_of * jnp.repeat(heights, dims[position] // shards_of).reshape([-1 if axis == position else 1 for axis in range(len(dims))])
    return factor_of


def shared_out(own_key, own, number, rows, number_of, top, bound, lean):
    sequence = jax.random.permutation(own_key, number_of)
    crowded, ordinary = load_shares(number_of, rows * top, bound, lean, True), load_shares(number_of, rows * top, bound, lean, False)
    places = jnp.arange(number_of)

    def named(sizes, offset_by):
        used = int((sizes > 0).sum())
        fixed = max(1, used // 4)
        moved = fixed + (places - fixed + offset_by * (used - fixed)) % max(1, number_of - fixed)
        return jnp.zeros((number_of,), jnp.int32).at[sequence[jnp.where(places < fixed, places, moved)]].set(jnp.asarray(sizes, jnp.int32))

    sizes = jnp.where(number % 4 == 0, named(crowded, number // 4), named(ordinary, number - number // 4 - 1))
    mixed = jax.random.permutation(jax.random.fold_in(own, 3), number_of)
    source_of, sink = mixed[0:number_of // 2 * 2:2], mixed[1:number_of // 2 * 2:2]
    slack = jnp.minimum(sizes[source_of] - 1, bound - sizes[sink]) // 2
    slack = jnp.where((source_of == sequence[0]) | (sink == sequence[0]) | (sizes[sink] == 0), 0, jnp.maximum(slack, 0))
    moved = jax.random.randint(jax.random.fold_in(own, 4), (number_of // 2,), 0, 1 << 20) % (slack + 1)
    sizes = sizes.at[source_of].add(-moved).at[sink].add(moved)
    items = jnp.searchsorted(jnp.cumsum(sizes), jnp.arange(rows * top), side="right").astype(jnp.int32)
    grid = items.reshape(top, rows).T
    grid = grid[jax.random.permutation(jax.random.fold_in(own, 1), rows)]
    offset_by = jax.random.randint(jax.random.fold_in(own, 2), (rows, 1), 0, top)
    return jnp.take_along_axis(grid, (jnp.arange(top)[None, :] + offset_by) % top, axis=1)


def load_shares(number_of, total, limit, lean, full):
    weights = [(1 << 20) // math.isqrt(grade ** lean) + 1 for grade in range(1, number_of + 1)]
    largest = limit if full else min(limit, max(-(-total // number_of), total * weights[0] // sum(weights)))
    least = 1 if total - largest >= number_of - 1 else 0
    given, rest = [largest] + [least] * (number_of - 1), total - largest - least * (number_of - 1)
    while rest > 0:
        movable = [i for i in range(1, number_of) if given[i] < largest] or [i for i in range(1, number_of) if given[i] < limit]
        whole, budget = sum([weights[i] for i in movable]), rest
        for i in movable:
            addition = min(limit - given[i], max(1, budget * weights[i] // whole), rest)
            given[i] = given[i] + addition
            rest = rest - addition
    return np.array(given)


def bell_draw(key, extent, width, most, split=(), kind=jnp.bfloat16):
    array = jax.random.normal(key, extent, jnp.float32) * width
    if len(split) > 0:
        array = level_of(key, extent, split, -0.22, 0.18) * array
    return jnp.clip(array, min=-most, max=most).astype(kind)


def setup_inputs(seed: int = 0) -> dict:
    streams_of = jax.random.split(jax.random.key(seed), 8)
    tokens = bell_draw(streams_of[0], (TOKENS, D), 1.0, 6.0, ((0, 16),))
    cotangent = bell_draw(streams_of[1], (TOKENS, D), 0.25, 1.5, ((0, 16),))
    gates = jnp.clip(0.05 + 0.9 * jax.random.uniform(streams_of[2], (TOKENS, TOPK), jnp.float32) ** level_of(streams_of[2], (TOKENS, TOPK), ((0, 16),), -0.2, 0.2), 0.05, 0.95)
    experts_keys = jax.random.split(jax.random.fold_in(streams_of[3], 1), TOKENS // TOK_DEV)
    experts_turns = jax.random.permutation(jax.random.fold_in(streams_of[3], 3), TOKENS // TOK_DEV)
    experts = jax.vmap(lambda own, number: shared_out(jax.random.fold_in(streams_of[3], 2), own, number, TOK_DEV, EXPERTS, TOPK, CAP, 2))(experts_keys, experts_turns).reshape((TOKENS, TOPK))
    gate_w = bell_draw(streams_of[4], (EXPERTS, D, FF), D ** -0.5, 0.09375, ((0, 16), (2, 2)))
    up_w = bell_draw(streams_of[5], (EXPERTS, D, FF), D ** -0.5, 0.09375, ((0, 16), (2, 2)))
    down_w = bell_draw(streams_of[6], (EXPERTS, FF, D), FF ** -0.5, 0.21875, ((0, 16), (1, 2)))
    return dict(tokens=tokens, cotangent=cotangent, gates=gates, experts=experts, gate_w=gate_w, up_w=up_w, down_w=down_w)


def expert_terms(w_gate, w_up, w_down, indices, tokens, cotangent, gates):
    n_assign = TOKENS * TOPK
    valid = indices < n_assign
    safe = jnp.minimum(indices, n_assign - 1)
    tok_index = safe // TOPK
    rows_x = jnp.where(valid[:, None], tokens[tok_index], jnp.zeros((), jnp.bfloat16)).astype(jnp.bfloat16)
    rows_dy = jnp.where(valid[:, None], cotangent[tok_index], jnp.zeros((), jnp.bfloat16)).astype(jnp.bfloat16)
    rows_g = jnp.where(valid, gates.reshape(-1)[safe], jnp.zeros((), jnp.float32))
    pre_gate = jnp.dot(rows_x, w_gate, preferred_element_type=jnp.float32)
    pre_up = jnp.dot(rows_x, w_up, preferred_element_type=jnp.float32)
    sigmoid_gate = jax.nn.sigmoid(pre_gate)
    silu_gate = pre_gate * sigmoid_gate
    hidden = (silu_gate * pre_up).astype(jnp.bfloat16)
    hidden_grad = jnp.dot(rows_dy, w_down.T, preferred_element_type=jnp.float32)
    gate_sum = jnp.sum(hidden.astype(jnp.float32) * hidden_grad, axis=1)
    scaled = rows_g[:, None] * hidden_grad
    grad_pre_gate = (scaled * pre_up * sigmoid_gate * (1.0 + pre_gate * (1.0 - sigmoid_gate))).astype(jnp.bfloat16)
    grad_pre_up = (scaled * silu_gate).astype(jnp.bfloat16)
    weighted = (rows_g[:, None] * hidden.astype(jnp.float32)).astype(jnp.bfloat16)
    grad_dw = jnp.dot(weighted.T, rows_dy, preferred_element_type=jnp.float32).astype(jnp.bfloat16)
    grad_gw = jnp.dot(rows_x.T, grad_pre_gate, preferred_element_type=jnp.float32).astype(jnp.bfloat16)
    grad_uw = jnp.dot(rows_x.T, grad_pre_up, preferred_element_type=jnp.float32).astype(jnp.bfloat16)
    rows = rows_x.shape[0]
    block_units = FF // N_TP
    split_gate = grad_pre_gate.astype(jnp.float32).reshape(rows, N_TP, block_units)
    split_up = grad_pre_up.astype(jnp.float32).reshape(rows, N_TP, block_units)
    wg_split = w_gate.astype(jnp.float32).reshape(D, N_TP, block_units)
    wu_split = w_up.astype(jnp.float32).reshape(D, N_TP, block_units)
    partial_value = jnp.einsum('rhf,dhf->rhd', split_gate, wg_split) + jnp.einsum('rhf,dhf->rhd', split_up, wu_split)
    partial_value = partial_value.astype(jnp.bfloat16).astype(jnp.float32)
    row_grad = jnp.sum(partial_value, axis=1).astype(jnp.bfloat16)
    return grad_gw, grad_uw, grad_dw, row_grad, gate_sum


def reference(tokens, cotangent, gates, experts, gate_w, up_w, down_w):
    n_assign = TOKENS * TOPK
    flat_ids = experts.reshape(N_EP, TOK_DEV * TOPK)
    onehot = (flat_ids[:, :, None] == jnp.arange(EXPERTS, dtype=jnp.int32)[None, None, :]).astype(jnp.int32)
    earlier = jnp.cumsum(onehot, axis=1) - onehot
    slot_of = jnp.sum(earlier * onehot, axis=2).astype(jnp.int32)
    block_id = jnp.broadcast_to(jnp.arange(N_EP, dtype=jnp.int32)[:, None], flat_ids.shape)
    numbers = jnp.arange(n_assign, dtype=jnp.int32).reshape(N_EP, TOK_DEV * TOPK)
    table = jnp.full((EXPERTS, N_EP, CAP), n_assign, jnp.int32).at[flat_ids, block_id, slot_of].set(numbers)
    table = table.reshape(EXPERTS, N_EP * CAP)

    def per_expert(args):
        w_gate, w_up, w_down, indices = args
        return expert_terms(w_gate, w_up, w_down, indices, tokens, cotangent, gates)

    grad_gw, grad_uw, grad_dw, row_grad, gate_sum = lax.map(per_expert, (gate_w, up_w, down_w, table))
    flat_index = table.reshape(-1)
    tok_target = jnp.where(flat_index < n_assign, flat_index // TOPK, TOKENS).astype(jnp.int32)
    grad_tokens = jnp.zeros((TOKENS, D), jnp.float32).at[tok_target].add(
        row_grad.reshape(-1, D).astype(jnp.float32), mode="drop").astype(jnp.bfloat16)
    grad_gates = jnp.zeros((n_assign,), jnp.float32).at[flat_index].set(
        gate_sum.reshape(-1), mode="drop").reshape(TOKENS, TOPK)
    gw_f = grad_gw.astype(jnp.float32)
    uw_f = grad_uw.astype(jnp.float32)
    dw_f = grad_dw.astype(jnp.float32)
    sq_gate = jnp.sum(gw_f * gw_f, axis=2) / FF
    sq_up = jnp.sum(uw_f * uw_f, axis=2) / FF
    sq_down = jnp.sum(dw_f * dw_f, axis=2) / D
    return (grad_tokens, grad_gates, grad_gw, grad_uw, grad_dw, sq_gate, sq_up, sq_down)
```

```python
import functools

import jax
import jax.numpy as jnp
from jax import lax
from jax.experimental import pallas as pl
from jax.experimental.pallas import tpu as pltpu
from jax.sharding import PartitionSpec as P

MESH = pl.DeviceIdType.MESH
BF16 = jnp.bfloat16
F32 = jnp.float32
NN = (((1,), (0,)), ((), ()))
NT = (((1,), (1,)), ((), ()))
TN = (((0,), (0,)), ((), ()))
VMEM_BYTES = 67043328
PLANES = 4


def dot(a, b, dims, precision=None):
    return lax.dot_general(a, b, dims, precision=precision, preferred_element_type=F32)


def kernel(
    n, cap, units, share, groups, tile,
    sx, sdy, sg, wg_in, wu_in, wd_in,
    back, gback, ggw, guw, gdw, sq_out, sqd_out,
    xr, dyr, gr, wg, wu, wd, pg, pu, prod, gpgu, wt, keep, give, got, rg,
    gp, gpp, gt, gcol, sqs, sqr, acc,
    w_sem, s_sem, r_sem, gs_sem, gr_sem, fs_sem, fr_sem,
    ps_sem, pr_sem, qs_sem, qr_sem, bs_sem, br_sem, hs_sem, hr_sem, o_sem, e_sem,
):
    me = lax.axis_index("ep")
    t = lax.axis_index("tp")
    other = lax.axis_size("tp") - 1 - t
    per = n // groups
    rows_g = per * cap

    def rows(s):
        return pl.ds(pl.multiple_of(s * cap, 16), cap)

    def remote(src, dst, send, recv, **where):
        return pltpu.make_async_remote_copy(
            src_ref=src, dst_ref=dst, send_sem=send, recv_sem=recv,
            device_id=where, device_id_type=MESH,
        )

    def loop(count, fn):
        def step(i, carry):
            fn(i)
            return carry
        lax.fori_loop(0, count, step, 0)

    def peer(k):
        return lax.rem(me + n // 2 + k + jnp.where(k >= n - n // 2, 1, 0), n)

    barrier = pltpu.get_barrier_semaphore()
    loop(n - 1, lambda k: pl.semaphore_signal(
        barrier, inc=1, device_id={"ep": peer(k)}, device_id_type=MESH))
    pl.semaphore_signal(barrier, inc=1, device_id={"tp": other}, device_id_type=MESH)
    pl.semaphore_wait(barrier, n)

    ins = ((sx, xr), (sdy, dyr))
    for which, (src, dst) in enumerate(ins):
        def send(k, which=which, src=src, dst=dst):
            d = peer(k)
            remote(src.at[d], dst.at[t, rows(me)], s_sem.at[which, d],
                   r_sem.at[which, me], ep=d).start()
        loop(n - 1, send)
        pltpu.make_async_copy(src.at[me], dst.at[t, rows(me)], r_sem.at[which, me]).start()
        if which == 0:
            def send_gate(k):
                d = peer(k)
                remote(sg.at[d], gr.at[me], gs_sem.at[d], gr_sem.at[me], ep=d).start()
            loop(n - 1, send_gate)
            pltpu.make_async_copy(sg.at[me], gr.at[me], gr_sem.at[me]).start()
            loads = [
                pltpu.make_async_copy(a, b, w_sem.at[i])
                for i, (a, b) in enumerate(((wg_in, wg), (wu_in, wu), (wd_in, wd)))
            ]
            for load in loads:
                load.start()

    def order(i):
        return lax.rem(me // per + groups // 2 + i, groups)

    def arrive(which, g):
        src, dst = ins[which]

        def pass_on(j):
            s = g * per + j
            pltpu.make_async_copy(src.at[0], dst.at[t, rows(s)], r_sem.at[which, s]).wait()
            remote(dst.at[t, rows(s)], dst.at[t, rows(s)], fs_sem.at[which, s],
                   fr_sem.at[which, s], tp=other).start()

        def joined(j):
            s = g * per + j
            remote(dst.at[other, rows(s)], dst.at[other, rows(s)], fs_sem.at[which, s],
                   fr_sem.at[which, s], tp=other).wait_recv()

        loop(per, pass_on)
        loop(per, joined)

    def span(g):
        return pl.ds(pl.multiple_of(g * rows_g, 16), rows_g)

    for load in loads:
        load.wait()

    def forward(i):
        g = order(i)
        arrive(0, g)
        r = span(g)
        pg[r, :] = dot(xr[0, r, :], wg[0], NN) + dot(xr[1, r, :], wg[1], NN)
        pu[r, :] = dot(xr[0, r, :], wu[0], NN) + dot(xr[1, r, :], wu[1], NN)

    loop(groups, forward)

    def exchange(g):
        r = span(g)
        grp = pl.ds(g * per, per)
        return (
            remote(give.at[r], got.at[r], ps_sem.at[g], pr_sem.at[g], tp=other),
            remote(gp.at[grp], gpp.at[grp], qs_sem.at[g], qr_sem.at[g], tp=other),
        )

    def back_copies(s):
        return (
            remote(rg.at[rows(s)], back.at[me], bs_sem.at[s], br_sem.at[me], ep=s),
            remote(gt.at[s], gback.at[me], hs_sem.at[s], hr_sem.at[me], ep=s),
        )

    def finish(g):
        for copy in exchange(g):
            copy.wait_recv()

        def one(j):
            s = g * per + j
            r = rows(s)
            rg[r, :] = (keep[r, :].astype(F32) + got[r, :].astype(F32)).astype(BF16)
            gt[s] = gp[s] + gpp[s]

        loop(per, one)

        def out(j):
            s = g * per + j

            @pl.when(s == me)
            def _():
                pltpu.make_async_copy(rg.at[rows(s)], back.at[me], br_sem.at[me]).start()
                pltpu.make_async_copy(gt.at[s], gback.at[me], hr_sem.at[me]).start()

            @pl.when(s != me)
            def _():
                for copy in back_copies(s):
                    copy.start()

        loop(per, out)

    ones_units = jnp.ones((8, units), F32)

    def backward(i):
        g = order(i)
        arrive(1, g)

        def gates_in(j):
            s = g * per + j
            pltpu.make_async_copy(sg.at[0], gr.at[s], gr_sem.at[s]).wait()
            column = jnp.transpose(gr[s])
            gcol[rows(s), :] = jnp.broadcast_to(column[:cap, 0:1], (cap, 128))

        loop(per, gates_in)
        r = span(g)
        dh = dot(dyr[0, r, :], wd[:, :share], NT) + dot(dyr[1, r, :], wd[:, share:], NT)
        a = pg[r, :]
        b = pu[r, :]
        gate = gcol[r, 0:1]
        sig = jax.nn.sigmoid(a)
        silu = a * sig
        hidden = (silu * b).astype(BF16).astype(F32)
        prod[...] = hidden * dh
        scaled = gate * dh
        gpg = (scaled * b * sig * (1.0 + a * (1.0 - sig))).astype(BF16)
        gpu = (scaled * silu).astype(BF16)
        gpgu[r, :units] = gpg
        gpgu[r, units:] = gpu
        wt[r, :] = (gate * hidden).astype(BF16)

        def part(c):
            cols = pl.ds(pl.multiple_of(c * tile, tile), tile)
            for half, dst in ((other, give), (t, keep)):
                dst[r, cols] = (
                    dot(gpgu[r, :units], wg[half, cols, :], NT)
                    + dot(gpgu[r, units:], wu[half, cols, :], NT)
                ).astype(BF16)

        loop(share // tile, part)

        def gate_sum(j):
            p = prod[pl.ds(pl.multiple_of(j * cap, 16), cap), :]
            gp[g * per + j, :, :cap] = dot(ones_units, p, NT, lax.Precision.HIGHEST)

        loop(per, gate_sum)
        for copy in exchange(g):
            copy.start()

        @pl.when(i > 0)
        def _():
            finish(order(i - 1 + groups))

    gp[...] = jnp.zeros_like(gp)
    loop(groups, backward)
    finish(order(groups - 1))

    acc[...] = jnp.zeros_like(acc)
    for h in range(2):
        def grads(c, h=h):
            cols = pl.ds(pl.multiple_of(c * tile, tile), tile)
            q = dot(xr[h, :, cols], gpgu[...], TN).astype(BF16)
            wg[h, cols, :] = q[:, :units]
            wu[h, cols, :] = q[:, units:]
            f = q.astype(F32)
            f = f * f
            sqs[0, h, c] = dot(ones_units, f[:, :units], NT, lax.Precision.HIGHEST)
            sqs[1, h, c] = dot(ones_units, f[:, units:], NT, lax.Precision.HIGHEST)
            d = dot(wt[...], dyr[h, :, cols], TN).astype(BF16)
            wd[:, pl.ds(pl.multiple_of(h * share + c * tile, tile), tile)] = d
            d = d.astype(F32)
            acc[...] += d * d

        loop(share // tile, grads)

    stores = [
        pltpu.make_async_copy(a, b, o_sem.at[i])
        for i, (a, b) in enumerate(((wg, ggw), (wu, guw), (wd, gdw)))
    ]
    for store in stores:
        store.start()
    squares = remote(sqs, sqr, e_sem.at[0], e_sem.at[1], tp=other)
    squares.start()
    sqd_out[...] = dot(jnp.ones((8, tile), F32), acc[...], NT, lax.Precision.HIGHEST)
    squares.wait()
    sq_out[...] = sqs[...] + sqr[...]
    for store in stores:
        store.wait()

    def drain(k):
        d = peer(k)
        for which, (src, dst) in enumerate(ins):
            remote(src.at[d], dst.at[t, rows(me)], s_sem.at[which, d],
                   r_sem.at[which, me], ep=d).wait_send()
        remote(sg.at[d], gr.at[me], gs_sem.at[d], gr_sem.at[me], ep=d).wait_send()
        for copy in back_copies(d):
            copy.wait_send()

    loop(n - 1, drain)

    def drain_pair(s):
        for which, (src, dst) in enumerate(ins):
            remote(dst.at[t, rows(s)], dst.at[t, rows(s)], fs_sem.at[which, s],
                   fr_sem.at[which, s], tp=other).wait_send()
        pltpu.make_async_copy(rg.at[rows(s)], back.at[s], br_sem.at[s]).wait()
        pltpu.make_async_copy(gt.at[s], gback.at[s], hr_sem.at[s]).wait()

    loop(n, drain_pair)

    def drain_group(g):
        for copy in exchange(g):
            copy.wait_send()

    loop(groups, drain_group)


def fused(n, cap, send_x, send_dy, send_gate, w_gate, w_up, w_down):
    width, units = w_gate.shape
    share = send_x.shape[2]
    total = n * cap
    groups = 4
    tile = 512
    any_spec = pl.BlockSpec(memory_space=pl.ANY)
    vmem = pl.BlockSpec(memory_space=pltpu.VMEM)
    sq_shape = (2, 2, share // tile, 8, tile)
    dma = pltpu.SemaphoreType.DMA
    shape = jax.ShapeDtypeStruct
    return pl.pallas_call(
        functools.partial(kernel, n, cap, units, share, groups, tile),
        out_shape=(
            shape((n, cap, share), BF16),
            shape((n, 8, 128), F32),
            shape((2, share, units), BF16),
            shape((2, share, units), BF16),
            shape((units, width), BF16),
            shape(sq_shape, F32),
            shape((8, units), F32),
        ),
        in_specs=[any_spec] * 6,
        out_specs=(any_spec,) * 5 + (vmem, vmem),
        scratch_shapes=[
            pltpu.VMEM((2, total, share), BF16),
            pltpu.VMEM((2, total, share), BF16),
            pltpu.VMEM((n, 8, 128), F32),
            pltpu.VMEM((2, share, units), BF16),
            pltpu.VMEM((2, share, units), BF16),
            pltpu.VMEM((units, width), BF16),
            pltpu.VMEM((total, units), F32),
            pltpu.VMEM((total, units), F32),
            pltpu.VMEM((total // groups, units), F32),
            pltpu.VMEM((total, 2 * units), BF16),
            pltpu.VMEM((total, units), BF16),
            pltpu.VMEM((total, share), BF16),
            pltpu.VMEM((total, share), BF16),
            pltpu.VMEM((total, share), BF16),
            pltpu.VMEM((total, share), BF16),
            pltpu.VMEM((n, 8, 128), F32),
            pltpu.VMEM((n, 8, 128), F32),
            pltpu.VMEM((n, 8, 128), F32),
            pltpu.VMEM((total, 128), F32),
            pltpu.VMEM(sq_shape, F32),
            pltpu.VMEM(sq_shape, F32),
            pltpu.VMEM((units, tile), F32),
            dma((3,)), dma((2, n)), dma((2, n)), dma((n,)), dma((n,)), dma((2, n)), dma((2, n)),
            dma((groups,)), dma((groups,)), dma((groups,)), dma((groups,)),
            dma((n,)), dma((n,)), dma((n,)), dma((n,)), dma((3,)), dma((2,)),
        ],
        compiler_params=pltpu.CompilerParams(
            collective_id=0, has_side_effects=True, vmem_limit_bytes=63 << 20
        ),
    )(send_x, send_dy, send_gate,
      w_gate.reshape(2, share, units), w_up.reshape(2, share, units), w_down)


def relay_kernel(
    n, planes, cap, units, share, tile, toks, full_units,
    tok, cot, gates, experts, wg_in, wu_in, wd_in,
    gtok, ggate, ggw, guw, gdw, sqg, squ, sqd,
    xd, tx, pn, near, tg, rt, pq, raw, fwd, wg, wu, wd, gs, gr, gcol, pg, pu, prod, gpgu, wt,
    give, got, rg, gp, gpp, gt, gback, back, comb, far, gout, sqs, sqr, acc,
    w_sem, t_sem, raw_s, raw_r, meta_s, meta_r, s_sem, r_sem, f_sem, gs_sem, gr_sem, ps_sem, pr_sem,
    xs_sem, xr_sem, qs_sem, qr_sem, bs_sem, br_sem, cs_sem, cr_sem, hs_sem, hr_sem, o_sem, e_sem, go_sem,
):
    me = lax.axis_index("ep")
    t = lax.axis_index("tp")
    other = lax.axis_size("tp") - 1 - t
    per = n // planes
    half = n // 2
    rows_g = per * cap
    hr = half * cap
    chunks = share // tile
    z = me // per
    col = me % per
    h = z // (planes // 2)
    oh = 1 - h
    first = h * half
    mine = me - first
    own_inner, own_outer = 1 + h, (planes - 1) * h
    far_inner, far_outer = 1 + oh, (planes - 1) * oh
    inner = z == own_inner
    my_relay = far_inner * per + col
    my_q = jnp.where(inner, 1, 0)

    def rows(s):
        return pl.ds(pl.multiple_of(s * cap, 16), cap)

    def cols_of(c):
        return pl.ds(pl.multiple_of(c * tile, tile), tile)

    def remote(src, dst, send, recv, **where):
        return pltpu.make_async_remote_copy(
            src_ref=src, dst_ref=dst, send_sem=send, recv_sem=recv,
            device_id=where, device_id_type=MESH,
        )

    def local(src, dst, sem):
        return pltpu.make_async_copy(src, dst, sem)

    def loop(count, fn):
        def step(i, carry):
            fn(i)
            return carry
        lax.fori_loop(0, count, step, 0)

    def peer(k):
        return lax.rem(me + n // 2 + k + jnp.where(k >= n - n // 2, 1, 0), n)

    barrier = pltpu.get_barrier_semaphore()
    loop(n - 1, lambda k: pl.semaphore_signal(
        barrier, inc=1, device_id={"ep": peer(k)}, device_id_type=MESH))
    pl.semaphore_signal(barrier, inc=1, device_id={"tp": other}, device_id_type=MESH)

    my_cols = pl.ds(pl.multiple_of(t * share, share), share)
    ins = (tok, cot)
    shares = [local(a.at[:, my_cols], tx.at[w], t_sem.at[w]) for w, a in enumerate(ins)]
    loads = [
        local(a, b, w_sem.at[i])
        for i, (a, b) in enumerate(((wg_in, wg), (wu_in, wu), (wd_in, wd)))
    ]
    for copy in shares:
        copy.start()

    e0, e1 = experts[0:1, :], experts[1:2, :]
    which_expert = lax.broadcasted_iota(jnp.int32, (n, toks), 0)
    hit0 = (which_expert == e0).astype(F32)
    hit1 = (which_expert == e1).astype(F32)
    before = (
        lax.broadcasted_iota(jnp.int32, (toks, toks), 0)
        < lax.broadcasted_iota(jnp.int32, (toks, toks), 1)
    ).astype(F32).astype(BF16)
    earlier = dot((hit0 + hit1).astype(BF16), before, NN)
    t0 = e0.astype(F32) * cap + jnp.sum(earlier * hit0, axis=0, keepdims=True)
    t1 = e1.astype(F32) * cap + jnp.sum(earlier * hit1, axis=0, keepdims=True)
    tg[0:1, :] = t0
    tg[1:2, :] = t1
    tg[2:4, :] = gates[...]
    tg[4:8, :] = jnp.zeros((4, toks), F32)

    half_rows = (lax.broadcasted_iota(jnp.int32, (hr, toks), 0) + first * cap).astype(F32)

    def placing(a, b):
        return jnp.where((half_rows == a) | (half_rows == b), 1.0, 0.0).astype(BF16)

    pn[...] = placing(t0, t1)

    pl.semaphore_wait(barrier, n)

    def raw_copy(which, c):
        at = pl.ds(pl.multiple_of(t * share + c * tile, tile), tile)
        return remote(ins[which].at[:, at], raw.at[my_q, which, :, cols_of(c)],
                      raw_s.at[which, c], raw_r.at[my_q, which, c], ep=my_relay)

    def raw_send():
        for which in range(2):
            loop(chunks, lambda c, which=which: raw_copy(which, c).start())

    meta = remote(tg, rt.at[my_q], meta_s.at[0], meta_r.at[my_q], ep=my_relay)
    meta.start()

    @pl.when(z == own_outer)
    def _():
        raw_send()

    def near_slot(k):
        return lax.rem(mine + per + k, half)

    def near_copy(which, d):
        return remote(near.at[which, rows(d)], xd.at[which, t, rows(me)], s_sem.at[which, d],
                      r_sem.at[which, me], ep=first + d)

    for which in range(2):
        shares[which].wait()

        def place(c, which=which):
            near[which, :, cols_of(c)] = dot(pn[...], tx[which, :, cols_of(c)], NN).astype(BF16)

        loop(chunks, place)

        def send(k, which=which):
            d = near_slot(k)

            @pl.when(d != mine)
            def _():
                near_copy(which, d).start()

            @pl.when(d == mine)
            def _():
                local(near.at[which, rows(d)], xd.at[which, t, rows(me)], r_sem.at[which, me]).start()

        loop(half, send)

    for load in loads:
        load.start()

    columns = jnp.transpose(tg[...])
    c0, c1, g0, g1 = (columns[:, i:i + 1] for i in range(4))
    lanes = lax.broadcasted_iota(jnp.int32, (toks, 128), 1)
    lanes = jnp.where(lanes < cap, lanes, -2 * n * cap).astype(F32)

    def gate_row(e):
        base = (e * cap).astype(F32)
        picked = jnp.where(c0 - base == lanes, g0, 0.0) + jnp.where(c1 - base == lanes, g1, 0.0)
        gs[e] = jnp.broadcast_to(jnp.sum(picked, axis=0, keepdims=True), (8, 128))

    loop(n, gate_row)

    def gate_copy(d):
        return remote(gs.at[d], gr.at[me], gs_sem.at[d], gr_sem.at[me], ep=d)

    loop(n - 1, lambda k: gate_copy(peer(k)).start())
    local(gs.at[me], gr.at[me], gr_sem.at[me]).start()

    def source_of(q):
        return jnp.where(q == 0, far_outer, far_inner) * per + col

    def fwd_copy(q, which, d, at):
        src = source_of(q)
        return remote(fwd.at[q, which, rows(d), at], xd.at[which, t, rows(src), at],
                      f_sem.at[q, which, d], r_sem.at[which, src], ep=first + d)

    def relay(q):
        src = source_of(q)
        remote(tg, rt.at[q], meta_s.at[0], meta_r.at[q], ep=my_relay).wait_recv()
        pq[q] = placing(rt[q, 0:1, :], rt[q, 1:2, :])

        def step(i):
            which = i // chunks
            c = i % chunks
            at = cols_of(c)
            remote(raw.at[q, which, :, at], raw.at[q, which, :, at], raw_s.at[0, 0],
                   raw_r.at[q, which, c], ep=my_relay).wait_recv()

            @pl.when((q == 0) & (i == 2 * chunks - 2))
            def _():
                raw_send()

            fwd[q, which, :, at] = dot(pq[q], raw[q, which, :, at], NN).astype(BF16)

            def pass_on(k):
                d = near_slot(k)

                @pl.when(d != mine)
                def _():
                    fwd_copy(q, which, d, at).start()

                @pl.when(d == mine)
                def _():
                    local(fwd.at[q, which, rows(d), at], xd.at[which, t, rows(src), at],
                          r_sem.at[which, src]).start()

            loop(half, pass_on)

        loop(2 * chunks, step)

    def pair_copy(which, s):
        block = xd.at[which, t, rows(s)]
        return remote(block, block, ps_sem.at[which, s], pr_sem.at[which, s], tp=other)

    def arrive(g):
        for which in range(2):
            def pass_on(j, which=which):
                s = g * per + j
                local(near.at[which, rows(0)], xd.at[which, t, rows(s)], r_sem.at[which, s]).wait()
                pair_copy(which, s).start()

            loop(per, pass_on)
        for which in range(2):
            def joined(j, which=which):
                s = g * per + j
                block = xd.at[which, other, rows(s)]
                remote(block, block, ps_sem.at[which, s], pr_sem.at[which, s], tp=other).wait_recv()

            loop(per, joined)

    ones_units = jnp.ones((8, units), F32)

    def exchange(g, c):
        block = (pl.ds(pl.multiple_of(g * rows_g, 16), rows_g), cols_of(c))
        return remote(give.at[block], got.at[block], xs_sem.at[g, c], xr_sem.at[g, c], tp=other)

    def gate_exchange(g):
        grp = pl.ds(g * per, per)
        return remote(gp.at[grp], gpp.at[grp], qs_sem.at[g], qr_sem.at[g], tp=other)

    def back_target(s):
        g = s // per
        close = g // (planes // 2) == h
        dest = jnp.where(close, s, own_inner * per + s % per)
        slot = jnp.where(close, 2, jnp.where(g == far_outer, 0, 1))
        return dest, slot

    def back_copy(s, c, at):
        dest, slot = back_target(s)
        return remote(rg.at[rows(s), at], back.at[slot, rows(mine), at], bs_sem.at[s],
                      br_sem.at[slot, c], ep=dest)

    def gate_back(s):
        return remote(gt.at[s], gback.at[me], hs_sem.at[s], hr_sem.at[me], ep=s)

    def group(g):
        arrive(g)
        r = pl.ds(pl.multiple_of(g * rows_g, 16), rows_g)
        pg[...] = dot(xd[0, 0, r, :], wg[0], NN) + dot(xd[0, 1, r, :], wg[1], NN)
        pu[...] = dot(xd[0, 0, r, :], wu[0], NN) + dot(xd[0, 1, r, :], wu[1], NN)

        def gates_in(j):
            s = g * per + j
            local(gs.at[0], gr.at[s], gr_sem.at[s]).wait()
            column = jnp.transpose(gr[s])
            gcol[rows(j), :] = jnp.broadcast_to(column[:cap, 0:1], (cap, 128))

        loop(per, gates_in)
        dh = dot(xd[1, 0, r, :], wd[:, :share], NT) + dot(xd[1, 1, r, :], wd[:, share:], NT)
        a = pg[...]
        b = pu[...]
        gate = gcol[:, 0:1]
        sig = jax.nn.sigmoid(a)
        silu = a * sig
        hidden = (silu * b).astype(BF16).astype(F32)
        prod[...] = hidden * dh
        scaled = gate * dh
        gpgu[r, :units] = (scaled * b * sig * (1.0 + a * (1.0 - sig))).astype(BF16)
        gpgu[r, units:] = (scaled * silu).astype(BF16)
        wt[r, :] = (gate * hidden).astype(BF16)

        def part(c):
            at = cols_of(c)
            for side, dst in ((other, give), (t, rg)):
                dst[r, at] = (
                    dot(gpgu[r, :units], wg[side, at, :], NT)
                    + dot(gpgu[r, units:], wu[side, at, :], NT)
                ).astype(BF16)
            exchange(g, c).start()

        def gate_sum(j):
            p = prod[rows(j), :]
            gp[g * per + j, :, :cap] = dot(ones_units, p, NT, lax.Precision.HIGHEST)

        def finish(c):
            at = cols_of(c)
            exchange(g, c).wait_recv()
            rg[r, at] = (rg[r, at].astype(F32) + got[r, at].astype(F32)).astype(BF16)

            def out(j):
                s = g * per + j
                dest, slot = back_target(s)

                @pl.when(dest == me)
                def _():
                    local(rg.at[rows(s), at], back.at[slot, rows(mine), at],
                          br_sem.at[slot, c]).start()

                @pl.when(dest != me)
                def _():
                    back_copy(s, c, at).start()

            loop(per, out)

        def column(c):
            @pl.when(c < chunks)
            def _():
                part(c)

            @pl.when(c > 0)
            def _():
                finish(c - 1)

        loop(chunks + 1, column)
        loop(per, gate_sum)
        gate_exchange(g).start()
        gate_exchange(g).wait_recv()

        def gates_out(j):
            s = g * per + j
            gt[s] = gp[s] + gpp[s]

            @pl.when(s == me)
            def _():
                local(gt.at[s], gback.at[me], hr_sem.at[me]).start()

            @pl.when(s != me)
            def _():
                gate_back(s).start()

        loop(per, gates_out)

    def comb_copy(q, at, c):
        return remote(comb.at[q, :, at], far.at[:, at], cs_sem.at[q, c], cr_sem.at[c],
                      ep=source_of(q))

    def combine(q, c):
        at = cols_of(c)
        local(near.at[0, :, at], back.at[q, :, at], br_sem.at[q, c]).wait()
        comb[q, :, at] = dot(pq[q], back[q, :, at], TN).astype(BF16)
        comb_copy(q, at, c).start()

    gp[...] = jnp.zeros_like(gp)
    for load in loads:
        load.wait()

    def phase(i):
        @pl.when(inner & (i % 2 == 0))
        def _():
            relay(i // 2)

        @pl.when(inner & (i == planes - 1))
        def _():
            loop(chunks, lambda c: combine(0, c))

        on_inner = jnp.where(i == 1, far_outer, jnp.where(i == 2, far_inner, own_outer))
        on_outer = jnp.where(i == 1, own_inner, jnp.where(i == 2, far_outer, far_inner))
        group(jnp.where(i == 0, z, jnp.where(inner, on_inner, on_outer)))

    loop(planes, phase)

    acc[...] = jnp.zeros_like(acc)

    def grads(i):
        side = i // chunks
        at = cols_of(i % chunks)
        wide = cols_of(i)
        q = dot(xd[0, side, :, at], gpgu[...], TN).astype(BF16)
        wg[side, at, :] = q[:, :units]
        wu[side, at, :] = q[:, units:]
        f = q.astype(F32)
        f = f * f
        sqs[0, :, wide] = dot(ones_units, f[:, :units], NT, lax.Precision.HIGHEST)
        sqs[1, :, wide] = dot(ones_units, f[:, units:], NT, lax.Precision.HIGHEST)
        d = dot(wt[...], xd[1, side, :, at], TN).astype(BF16)
        wd[:, wide] = d
        d = d.astype(F32)
        acc[...] += d * d

        @pl.when(inner & (i % 2 == 1))
        def _():
            combine(1, i // 2)

    loop(2 * chunks, grads)

    stores = [
        local(a, b, o_sem.at[i])
        for i, (a, b) in enumerate(((wg, ggw), (wu, guw), (wd, gdw)))
    ]
    for store in stores:
        store.start()
    squares = remote(sqs, sqr, e_sem.at[0], e_sem.at[1], tp=other)
    squares.start()
    sum_down = dot(jnp.ones((8, tile), F32), acc[...], NT, lax.Precision.HIGHEST)
    sqd[...] = sum_down[0:1, :] / (2 * share)
    squares.wait()
    sqg[...] = (sqs[0, 0:1, :] + sqr[0, 0:1, :]) / full_units
    squ[...] = (sqs[1, 0:1, :] + sqr[1, 0:1, :]) / full_units

    loop(n, lambda e: local(gt.at[e], gback.at[e], hr_sem.at[e]).wait())
    slots = lax.broadcasted_iota(jnp.int32, (cap, toks), 0)

    def look_up(e, carry):
        column = jnp.transpose(gback[e])[:cap, 0:1]
        at = (slots + e * cap).astype(F32)
        return tuple(
            v + jnp.where(at == tg[k:k + 1, :], column, 0.0) for k, v in enumerate(carry)
        )

    zero = jnp.zeros((cap, toks), F32)
    found = lax.fori_loop(0, n, look_up, (zero, zero))
    for k in range(2):
        ggate[k:k + 1, :] = jnp.sum(found[k], axis=0, keepdims=True)

    def last(c):
        at = cols_of(c)
        local(near.at[0, :, at], back.at[2, :, at], br_sem.at[2, c]).wait()
        close = dot(pn[...], back[2, :, at], TN)
        local(far.at[:, at], far.at[:, at], cr_sem.at[c]).wait()
        gout[:, at] = (close + far[:, at].astype(F32)).astype(BF16)
        local(gout.at[:, at], gtok.at[:, at], go_sem.at[c]).start()

    loop(chunks, last)

    for store in stores:
        store.wait()
    loop(chunks, lambda c: local(gout.at[:, cols_of(c)], gtok.at[:, cols_of(c)], go_sem.at[c]).wait())

    meta.wait_send()
    for which in range(2):
        loop(chunks, lambda c, which=which: raw_copy(which, c).wait_send())

    def drain_near(d):
        @pl.when(d != mine)
        def _():
            for which in range(2):
                near_copy(which, d).wait_send()

            @pl.when(inner)
            def _():
                for q in range(2):
                    for which in range(2):
                        fwd_copy(q, which, d, pl.ds(0, share)).wait_send()

    loop(half, drain_near)

    def drain(k):
        d = peer(k)
        gate_copy(d).wait_send()
        gate_back(d).wait_send()

    loop(n - 1, drain)

    def drain_rows(s):
        for which in range(2):
            pair_copy(which, s).wait_send()
        dest, _ = back_target(s)

        @pl.when(dest != me)
        def _():
            back_copy(s, 0, pl.ds(0, share)).wait_send()

    loop(n, drain_rows)

    def drain_group(g):
        loop(chunks, lambda c: exchange(g, c).wait_send())
        gate_exchange(g).wait_send()

    loop(planes, drain_group)

    @pl.when(inner)
    def _():
        for q in range(2):
            loop(chunks, lambda c, q=q: comb_copy(q, cols_of(c), c).wait_send())


def relay_scratch(n, planes, cap, units, share, tile, toks):
    total = n * cap
    group = total // planes
    hr = n // 2 * cap
    chunks = share // tile
    half = n // 2
    width = 2 * share
    arrays = [
        ((2, 2, total, share), BF16), ((2, toks, share), BF16), ((hr, toks), BF16),
        ((2, hr, share), BF16), ((8, toks), F32), ((2, 8, toks), F32), ((2, hr, toks), BF16),
        ((2, 2, toks, share), BF16), ((2, 2, hr, share), BF16),
        ((2, share, units), BF16), ((2, share, units), BF16), ((units, width), BF16),
        ((n, 8, 128), F32), ((n, 8, 128), F32), ((group, 128), F32),
        ((group, units), F32), ((group, units), F32), ((group, units), F32),
        ((total, 2 * units), BF16), ((total, units), BF16),
        ((total, share), BF16), ((total, share), BF16), ((total, share), BF16),
        ((n, 8, 128), F32), ((n, 8, 128), F32), ((n, 8, 128), F32), ((n, 8, 128), F32),
        ((3, hr, share), BF16), ((2, toks, share), BF16), ((toks, share), BF16),
        ((toks, share), BF16), ((2, 8, width), F32), ((2, 8, width), F32), ((units, tile), F32),
    ]
    sems = [
        (3,), (2,), (2, chunks), (2, 2, chunks), (1,), (2,), (2, half), (2, n), (2, 2, half),
        (n,), (n,), (2, n), (2, n), (planes, chunks), (planes, chunks), (planes,), (planes,),
        (n,), (3, chunks), (2, chunks), (chunks,), (n,), (n,), (3,), (2,), (chunks,),
    ]
    size = 0
    for dims, kind in arrays:
        count = jnp.dtype(kind).itemsize
        for d in dims:
            count *= d
        size += count
    return arrays, sems, size


def fused_relay(n, planes, cap, toks, tile, tokens, cotangent, gates, experts, w_gate, w_up, w_down):
    width, units = w_gate.shape
    cores = lax.axis_size("tp")
    share = width // cores
    any_spec = pl.BlockSpec(memory_space=pl.ANY)
    vmem = pl.BlockSpec(memory_space=pltpu.VMEM)
    shape = jax.ShapeDtypeStruct
    arrays, sems, _ = relay_scratch(n, planes, cap, units, share, tile, toks)
    return pl.pallas_call(
        functools.partial(relay_kernel, n, planes, cap, units, share, tile, toks, units * cores),
        out_shape=(
            shape((toks, share), BF16),
            shape((2, toks), F32),
            shape((2, share, units), BF16),
            shape((2, share, units), BF16),
            shape((units, width), BF16),
            shape((1, width), F32),
            shape((1, width), F32),
            shape((1, units), F32),
        ),
        in_specs=[any_spec, any_spec, vmem, vmem, any_spec, any_spec, any_spec],
        out_specs=(any_spec, vmem, any_spec, any_spec, any_spec, vmem, vmem, vmem),
        scratch_shapes=[pltpu.VMEM(dims, kind) for dims, kind in arrays]
        + [pltpu.SemaphoreType.DMA(dims) for dims in sems],
        compiler_params=pltpu.CompilerParams(
            collective_id=0, has_side_effects=True, vmem_limit_bytes=VMEM_BYTES
        ),
    )(tokens, cotangent, gates.T, experts.T,
      w_gate.reshape(2, share, units), w_up.reshape(2, share, units), w_down)


def body(tokens, cotangent, gates, experts, gate_w, up_w, down_w):
    tok_rows, width = tokens.shape
    top_count = experts.shape[1]
    n_ep = lax.axis_size("ep")
    n_cores = lax.axis_size("tp")
    capacity = 3 * tok_rows * top_count // (2 * n_ep)
    cap = -(-capacity // 16) * 16
    n_slots = n_ep * cap
    share = width // n_cores
    tile = 512
    units = gate_w.shape[2]
    _, _, size = relay_scratch(n_ep, PLANES, cap, units, share, tile, tok_rows)
    if n_ep % PLANES == 0 and tok_rows < n_ep // 2 * cap and size + (3 << 20) < VMEM_BYTES:
        gtok, ggate, ggw, guw, gdw, sqg, squ, sqd = fused_relay(
            n_ep, PLANES, cap, tok_rows, tile, tokens, cotangent, gates, experts,
            gate_w[0], up_w[0], down_w[0],
        )
        return (
            gtok, ggate.T, ggw.reshape(gate_w.shape), guw.reshape(up_w.shape), gdw[None],
            sqg, squ, sqd,
        )
    flat_ids = experts.reshape(-1)
    onehot = (flat_ids[:, None] == jnp.arange(n_ep, dtype=jnp.int32)[None, :]).astype(jnp.int32)
    earlier = jnp.cumsum(onehot, axis=0) - onehot
    slot_of = jnp.sum(earlier * onehot, axis=1)
    target = flat_ids * cap + slot_of
    placing = (target[None, :] == jnp.arange(n_slots, dtype=jnp.int32)[:, None]).astype(F32)
    place_tok = jnp.sum(placing.reshape(n_slots, tok_rows, top_count), axis=2).astype(BF16)
    send_gate = jnp.dot(placing, gates.reshape(-1), precision=lax.Precision.HIGHEST)
    send_gate = jnp.pad(send_gate.reshape(n_ep, 1, cap), ((0, 0), (0, 7), (0, 128 - cap)))
    share = width // n_cores
    offset = lax.axis_index("tp") * share
    tok_share = lax.dynamic_slice_in_dim(tokens, offset, share, 1)
    cot_share = lax.dynamic_slice_in_dim(cotangent, offset, share, 1)
    send_x = jnp.dot(place_tok, tok_share, preferred_element_type=F32).astype(BF16)
    send_dy = jnp.dot(place_tok, cot_share, preferred_element_type=F32).astype(BF16)
    back, gback, ggw, guw, gdw, sq, sqd = fused(
        n_ep, cap, send_x.reshape(n_ep, cap, share), send_dy.reshape(n_ep, cap, share),
        send_gate, gate_w[0], up_w[0], down_w[0],
    )
    grad_tokens = lax.dot_general(
        place_tok, back.reshape(n_slots, share), TN, preferred_element_type=F32
    ).astype(BF16)
    grad_gates = jnp.dot(
        gback[:, 0, :cap].reshape(n_slots), placing, precision=lax.Precision.HIGHEST
    ).reshape(tok_rows, top_count)
    full_units = gate_w.shape[2] * n_cores
    sq = sq[:, :, :, 0, :].reshape(2, width) / full_units
    return (
        grad_tokens,
        grad_gates,
        ggw.reshape(gate_w.shape),
        guw.reshape(up_w.shape),
        gdw[None],
        sq[0][None],
        sq[1][None],
        sqd[0:1] / width,
    )


def solution(mesh):
    placed = (
        P("ep", None),
        P("ep", None),
        P("ep", None),
        P("ep", None),
        P("ep", None, "tp"),
        P("ep", None, "tp"),
        P("ep", "tp", None),
    )
    return jax.shard_map(
        body,
        mesh=mesh,
        in_specs=placed,
        out_specs=(
            P("ep", "tp"),
            P("ep", None),
            P("ep", None, "tp"),
            P("ep", None, "tp"),
            P("ep", "tp", None),
            P("ep", None),
            P("ep", None),
            P("ep", "tp"),
        ),
        check_vma=False,
    )
```

```python
import functools

import jax
import jax.numpy as jnp
from jax import lax
from jax.experimental import pallas as pl
from jax.experimental.pallas import tpu as pltpu
from jax.sharding import PartitionSpec as P

MESH = pl.DeviceIdType.MESH
BF16 = jnp.bfloat16
F32 = jnp.float32
NN = (((1,), (0,)), ((), ()))
NT = (((1,), (1,)), ((), ()))
TN = (((0,), (0,)), ((), ()))
VMEM_BYTES = 67043328
PLANES = 4


def dot(a, b, dims, precision=None):
    return lax.dot_general(a, b, dims, precision=precision, preferred_element_type=F32)


def kernel(
    n, cap, units, share, groups, tile,
    sx, sdy, sg, wg_in, wu_in, wd_in,
    back, gback, ggw, guw, gdw, sq_out, sqd_out,
    xr, dyr, gr, wg, wu, wd, pg, pu, prod, gpgu, wt, keep, give, got, rg,
    gp, gpp, gt, gcol, sqs, sqr, acc,
    w_sem, s_sem, r_sem, gs_sem, gr_sem, fs_sem, fr_sem,
    ps_sem, pr_sem, qs_sem, qr_sem, bs_sem, br_sem, hs_sem, hr_sem, o_sem, e_sem,
):
    me = lax.axis_index("ep")
    t = lax.axis_index("tp")
    other = lax.axis_size("tp") - 1 - t
    per = n // groups
    rows_g = per * cap

    def rows(s):
        return pl.ds(pl.multiple_of(s * cap, 16), cap)

    def remote(src, dst, send, recv, **where):
        return pltpu.make_async_remote_copy(
            src_ref=src, dst_ref=dst, send_sem=send, recv_sem=recv,
            device_id=where, device_id_type=MESH,
        )

    def loop(count, fn):
        def step(i, carry):
            fn(i)
            return carry
        lax.fori_loop(0, count, step, 0)

    def peer(k):
        return lax.rem(me + n // 2 + k + jnp.where(k >= n - n // 2, 1, 0), n)

    barrier = pltpu.get_barrier_semaphore()
    loop(n - 1, lambda k: pl.semaphore_signal(
        barrier, inc=1, device_id={"ep": peer(k)}, device_id_type=MESH))
    pl.semaphore_signal(barrier, inc=1, device_id={"tp": other}, device_id_type=MESH)
    pl.semaphore_wait(barrier, n)

    ins = ((sx, xr), (sdy, dyr))
    for which, (src, dst) in enumerate(ins):
        def send(k, which=which, src=src, dst=dst):
            d = peer(k)
            remote(src.at[d], dst.at[t, rows(me)], s_sem.at[which, d],
                   r_sem.at[which, me], ep=d).start()
        loop(n - 1, send)
        pltpu.make_async_copy(src.at[me], dst.at[t, rows(me)], r_sem.at[which, me]).start()
        if which == 0:
            def send_gate(k):
                d = peer(k)
                remote(sg.at[d], gr.at[me], gs_sem.at[d], gr_sem.at[me], ep=d).start()
            loop(n - 1, send_gate)
            pltpu.make_async_copy(sg.at[me], gr.at[me], gr_sem.at[me]).start()
            loads = [
                pltpu.make_async_copy(a, b, w_sem.at[i])
                for i, (a, b) in enumerate(((wg_in, wg), (wu_in, wu), (wd_in, wd)))
            ]
            for load in loads:
                load.start()

    def order(i):
        return lax.rem(me // per + groups // 2 + i, groups)

    def arrive(which, g):
        src, dst = ins[which]

        def pass_on(j):
            s = g * per + j
            pltpu.make_async_copy(src.at[0], dst.at[t, rows(s)], r_sem.at[which, s]).wait()
            remote(dst.at[t, rows(s)], dst.at[t, rows(s)], fs_sem.at[which, s],
                   fr_sem.at[which, s], tp=other).start()

        def joined(j):
            s = g * per + j
            remote(dst.at[other, rows(s)], dst.at[other, rows(s)], fs_sem.at[which, s],
                   fr_sem.at[which, s], tp=other).wait_recv()

        loop(per, pass_on)
        loop(per, joined)

    def span(g):
        return pl.ds(pl.multiple_of(g * rows_g, 16), rows_g)

    for load in loads:
        load.wait()

    def forward(i):
        g = order(i)
        arrive(0, g)
        r = span(g)
        pg[r, :] = dot(xr[0, r, :], wg[0], NN) + dot(xr[1, r, :], wg[1], NN)
        pu[r, :] = dot(xr[0, r, :], wu[0], NN) + dot(xr[1, r, :], wu[1], NN)

    loop(groups, forward)

    def exchange(g):
        r = span(g)
        grp = pl.ds(g * per, per)
        return (
            remote(give.at[r], got.at[r], ps_sem.at[g], pr_sem.at[g], tp=other),
            remote(gp.at[grp], gpp.at[grp], qs_sem.at[g], qr_sem.at[g], tp=other),
        )

    def back_copies(s):
        return (
            remote(rg.at[rows(s)], back.at[me], bs_sem.at[s], br_sem.at[me], ep=s),
            remote(gt.at[s], gback.at[me], hs_sem.at[s], hr_sem.at[me], ep=s),
        )

    def finish(g):
        for copy in exchange(g):
            copy.wait_recv()

        def one(j):
            s = g * per + j
            r = rows(s)
            rg[r, :] = (keep[r, :].astype(F32) + got[r, :].astype(F32)).astype(BF16)
            gt[s] = gp[s] + gpp[s]

        loop(per, one)

        def out(j):
            s = g * per + j

            @pl.when(s == me)
            def _():
                pltpu.make_async_copy(rg.at[rows(s)], back.at[me], br_sem.at[me]).start()
                pltpu.make_async_copy(gt.at[s], gback.at[me], hr_sem.at[me]).start()

            @pl.when(s != me)
            def _():
                for copy in back_copies(s):
                    copy.start()

        loop(per, out)

    ones_units = jnp.ones((8, units), F32)

    def backward(i):
        g = order(i)
        arrive(1, g)

        def gates_in(j):
            s = g * per + j
            pltpu.make_async_copy(sg.at[0], gr.at[s], gr_sem.at[s]).wait()
            column = jnp.transpose(gr[s])
            gcol[rows(s), :] = jnp.broadcast_to(column[:cap, 0:1], (cap, 128))

        loop(per, gates_in)
        r = span(g)
        dh = dot(dyr[0, r, :], wd[:, :share], NT) + dot(dyr[1, r, :], wd[:, share:], NT)
        a = pg[r, :]
        b = pu[r, :]
        gate = gcol[r, 0:1]
        sig = jax.nn.sigmoid(a)
        silu = a * sig
        hidden = (silu * b).astype(BF16).astype(F32)
        prod[...] = hidden * dh
        scaled = gate * dh
        gpg = (scaled * b * sig * (1.0 + a * (1.0 - sig))).astype(BF16)
        gpu = (scaled * silu).astype(BF16)
        gpgu[r, :units] = gpg
        gpgu[r, units:] = gpu
        wt[r, :] = (gate * hidden).astype(BF16)

        def part(c):
            cols = pl.ds(pl.multiple_of(c * tile, tile), tile)
            for half, dst in ((other, give), (t, keep)):
                dst[r, cols] = (
                    dot(gpgu[r, :units], wg[half, cols, :], NT)
                    + dot(gpgu[r, units:], wu[half, cols, :], NT)
                ).astype(BF16)

        loop(share // tile, part)

        def gate_sum(j):
            p = prod[pl.ds(pl.multiple_of(j * cap, 16), cap), :]
            gp[g * per + j, :, :cap] = dot(ones_units, p, NT, lax.Precision.HIGHEST)

        loop(per, gate_sum)
        for copy in exchange(g):
            copy.start()

        @pl.when(i > 0)
        def _():
            finish(order(i - 1 + groups))

    gp[...] = jnp.zeros_like(gp)
    loop(groups, backward)
    finish(order(groups - 1))

    acc[...] = jnp.zeros_like(acc)
    for h in range(2):
        def grads(c, h=h):
            cols = pl.ds(pl.multiple_of(c * tile, tile), tile)
            q = dot(xr[h, :, cols], gpgu[...], TN).astype(BF16)
            wg[h, cols, :] = q[:, :units]
            wu[h, cols, :] = q[:, units:]
            f = q.astype(F32)
            f = f * f
            sqs[0, h, c] = dot(ones_units, f[:, :units], NT, lax.Precision.HIGHEST)
            sqs[1, h, c] = dot(ones_units, f[:, units:], NT, lax.Precision.HIGHEST)
            d = dot(wt[...], dyr[h, :, cols], TN).astype(BF16)
            wd[:, pl.ds(pl.multiple_of(h * share + c * tile, tile), tile)] = d
            d = d.astype(F32)
            acc[...] += d * d

        loop(share // tile, grads)

    stores = [
        pltpu.make_async_copy(a, b, o_sem.at[i])
        for i, (a, b) in enumerate(((wg, ggw), (wu, guw), (wd, gdw)))
    ]
    for store in stores:
        store.start()
    squares = remote(sqs, sqr, e_sem.at[0], e_sem.at[1], tp=other)
    squares.start()
    sqd_out[...] = dot(jnp.ones((8, tile), F32), acc[...], NT, lax.Precision.HIGHEST)
    squares.wait()
    sq_out[...] = sqs[...] + sqr[...]
    for store in stores:
        store.wait()

    def drain(k):
        d = peer(k)
        for which, (src, dst) in enumerate(ins):
            remote(src.at[d], dst.at[t, rows(me)], s_sem.at[which, d],
                   r_sem.at[which, me], ep=d).wait_send()
        remote(sg.at[d], gr.at[me], gs_sem.at[d], gr_sem.at[me], ep=d).wait_send()
        for copy in back_copies(d):
            copy.wait_send()

    loop(n - 1, drain)

    def drain_pair(s):
        for which, (src, dst) in enumerate(ins):
            remote(dst.at[t, rows(s)], dst.at[t, rows(s)], fs_sem.at[which, s],
                   fr_sem.at[which, s], tp=other).wait_send()
        pltpu.make_async_copy(rg.at[rows(s)], back.at[s], br_sem.at[s]).wait()
        pltpu.make_async_copy(gt.at[s], gback.at[s], hr_sem.at[s]).wait()

    loop(n, drain_pair)

    def drain_group(g):
        for copy in exchange(g):
            copy.wait_send()

    loop(groups, drain_group)


def fused(n, cap, send_x, send_dy, send_gate, w_gate, w_up, w_down):
    width, units = w_gate.shape
    share = send_x.shape[2]
    total = n * cap
    groups = 4
    tile = 512
    any_spec = pl.BlockSpec(memory_space=pl.ANY)
    vmem = pl.BlockSpec(memory_space=pltpu.VMEM)
    sq_shape = (2, 2, share // tile, 8, tile)
    dma = pltpu.SemaphoreType.DMA
    shape = jax.ShapeDtypeStruct
    return pl.pallas_call(
        functools.partial(kernel, n, cap, units, share, groups, tile),
        out_shape=(
            shape((n, cap, share), BF16),
            shape((n, 8, 128), F32),
            shape((2, share, units), BF16),
            shape((2, share, units), BF16),
            shape((units, width), BF16),
            shape(sq_shape, F32),
            shape((8, units), F32),
        ),
        in_specs=[any_spec] * 6,
        out_specs=(any_spec,) * 5 + (vmem, vmem),
        scratch_shapes=[
            pltpu.VMEM((2, total, share), BF16),
            pltpu.VMEM((2, total, share), BF16),
            pltpu.VMEM((n, 8, 128), F32),
            pltpu.VMEM((2, share, units), BF16),
            pltpu.VMEM((2, share, units), BF16),
            pltpu.VMEM((units, width), BF16),
            pltpu.VMEM((total, units), F32),
            pltpu.VMEM((total, units), F32),
            pltpu.VMEM((total // groups, units), F32),
            pltpu.VMEM((total, 2 * units), BF16),
            pltpu.VMEM((total, units), BF16),
            pltpu.VMEM((total, share), BF16),
            pltpu.VMEM((total, share), BF16),
            pltpu.VMEM((total, share), BF16),
            pltpu.VMEM((total, share), BF16),
            pltpu.VMEM((n, 8, 128), F32),
            pltpu.VMEM((n, 8, 128), F32),
            pltpu.VMEM((n, 8, 128), F32),
            pltpu.VMEM((total, 128), F32),
            pltpu.VMEM(sq_shape, F32),
            pltpu.VMEM(sq_shape, F32),
            pltpu.VMEM((units, tile), F32),
            dma((3,)), dma((2, n)), dma((2, n)), dma((n,)), dma((n,)), dma((2, n)), dma((2, n)),
            dma((groups,)), dma((groups,)), dma((groups,)), dma((groups,)),
            dma((n,)), dma((n,)), dma((n,)), dma((n,)), dma((3,)), dma((2,)),
        ],
        compiler_params=pltpu.CompilerParams(
            collective_id=0, has_side_effects=True, vmem_limit_bytes=63 << 20
        ),
    )(send_x, send_dy, send_gate,
      w_gate.reshape(2, share, units), w_up.reshape(2, share, units), w_down)


def relay_kernel(
    n, planes, cap, units, share, tile, toks, full_units,
    tok, cot, gates, experts, wg_in, wu_in, wd_in,
    gtok, ggate, ggw, guw, gdw, sqg, squ, sqd,
    xd, tx, pn, near, tg, rt, pq, raw, fwd, wg, wu, wd, gs, gr, gcol, pg, pu, prod, gpgu, wt,
    give, got, rg, gp, gpp, gt, gback, back, comb, far, mid, pm, sqs, sqr, acc,
    w_sem, t_sem, raw_s, raw_r, meta_s, meta_r, s_sem, r_sem, f_sem, gs_sem, gr_sem, ps_sem, pr_sem,
    xs_sem, xr_sem, qs_sem, qr_sem, bs_sem, br_sem, cs_sem, cr_sem, hs_sem, hr_sem, o_sem, e_sem, go_sem,
    n_sem, ms_sem, mr_sem, bf_sem, bg_sem,
):
    me = lax.axis_index("ep")
    t = lax.axis_index("tp")
    other = lax.axis_size("tp") - 1 - t
    per = n // planes
    half = n // 2
    rows_g = per * cap
    hr = half * cap
    chunks = share // tile
    z = me // per
    col = me % per
    h = z // (planes // 2)
    oh = 1 - h
    first = h * half
    mine = me - first
    own_inner, own_outer = 1 + h, (planes - 1) * h
    far_inner, far_outer = 1 + oh, (planes - 1) * oh
    inner = z == own_inner
    outer = z == own_outer
    next_plane = own_inner + own_outer - z
    my_relay = far_inner * per + col
    my_q = jnp.where(inner, 1, 0)

    def rows(s):
        return pl.ds(pl.multiple_of(s * cap, 16), cap)

    def cols_of(c):
        return pl.ds(pl.multiple_of(c * tile, tile), tile)

    def remote(src, dst, send, recv, **where):
        return pltpu.make_async_remote_copy(
            src_ref=src, dst_ref=dst, send_sem=send, recv_sem=recv,
            device_id=where, device_id_type=MESH,
        )

    def local(src, dst, sem):
        return pltpu.make_async_copy(src, dst, sem)

    def loop(count, fn):
        def step(i, carry):
            fn(i)
            return carry
        lax.fori_loop(0, count, step, 0)

    def peer(k):
        return lax.rem(me + n // 2 + k + jnp.where(k >= n - n // 2, 1, 0), n)

    barrier = pltpu.get_barrier_semaphore()
    loop(n - 1, lambda k: pl.semaphore_signal(
        barrier, inc=1, device_id={"ep": peer(k)}, device_id_type=MESH))
    pl.semaphore_signal(barrier, inc=1, device_id={"tp": other}, device_id_type=MESH)

    my_cols = pl.ds(pl.multiple_of(t * share, share), share)
    ins = (tok, cot)
    shares = [local(a.at[:, my_cols], tx.at[w], t_sem.at[w]) for w, a in enumerate(ins)]
    loads = [
        local(a, b, w_sem.at[i])
        for i, (a, b) in enumerate(((wg_in, wg), (wu_in, wu), (wd_in, wd)))
    ]
    for copy in shares:
        copy.start()

    e0, e1 = experts[0:1, :], experts[1:2, :]
    which_expert = lax.broadcasted_iota(jnp.int32, (n, toks), 0)
    hit0 = (which_expert == e0).astype(F32)
    hit1 = (which_expert == e1).astype(F32)
    before = (
        lax.broadcasted_iota(jnp.int32, (toks, toks), 0)
        < lax.broadcasted_iota(jnp.int32, (toks, toks), 1)
    ).astype(F32).astype(BF16)
    earlier = dot((hit0 + hit1).astype(BF16), before, NN)
    t0 = e0.astype(F32) * cap + jnp.sum(earlier * hit0, axis=0, keepdims=True)
    t1 = e1.astype(F32) * cap + jnp.sum(earlier * hit1, axis=0, keepdims=True)
    tg[0:1, :] = t0
    tg[1:2, :] = t1
    tg[2:4, :] = gates[...]
    tg[4:8, :] = jnp.zeros((4, toks), F32)

    half_rows = (lax.broadcasted_iota(jnp.int32, (hr, toks), 0) + first * cap).astype(F32)

    def placing(a, b):
        return jnp.where((half_rows == a) | (half_rows == b), 1.0, 0.0).astype(BF16)

    pn[...] = placing(t0, t1)

    columns = jnp.transpose(tg[...])
    c0, c1, g0, g1 = (columns[:, i:i + 1] for i in range(4))
    lanes = lax.broadcasted_iota(jnp.int32, (toks, 128), 1)
    lanes = jnp.where(lanes < cap, lanes, -2 * n * cap).astype(F32)

    def gate_row(e):
        base = (e * cap).astype(F32)
        picked = jnp.where(c0 - base == lanes, g0, 0.0) + jnp.where(c1 - base == lanes, g1, 0.0)
        gs[e, 0:1, :] = jnp.sum(picked, axis=0, keepdims=True)

    loop(n, gate_row)

    pl.semaphore_wait(barrier, n)

    def raw_copy(which, c):
        at = pl.ds(pl.multiple_of(t * share + c * tile, tile), tile)
        return remote(ins[which].at[:, at], raw.at[my_q, which, :, cols_of(c)],
                      raw_s.at[which, c], raw_r.at[my_q, which, c], ep=my_relay)

    def raw_send():
        for which in range(2):
            loop(chunks, lambda c, which=which: raw_copy(which, c).start())

    first_row = pl.ds(0, 1)

    def gate_copy(d):
        return remote(gs.at[d, first_row], gr.at[me, first_row], gs_sem.at[d], gr_sem.at[me], ep=d)

    loop(n - 1, lambda k: gate_copy(peer(k)).start())
    local(gs.at[me, first_row], gr.at[me, first_row], gr_sem.at[me]).start()

    meta = remote(tg, rt.at[my_q], meta_s.at[0], meta_r.at[my_q], ep=my_relay)
    meta.start()
    close_meta = remote(tg, rt.at[2], meta_s.at[1], meta_r.at[2], ep=own_inner * per + col)

    @pl.when(outer)
    def _():
        close_meta.start()

    @pl.when(outer)
    def _():
        raw_send()

    def near_copy(which, j):
        return remote(near.at[which, rows(z * per - first + j)], xd.at[which, t, rows(me)],
                      s_sem.at[which, j], r_sem.at[which, me], ep=z * per + j)

    def next_copy(which, c, at):
        return remote(near.at[which, next_block, at], raw.at[2, which, block, at],
                      n_sem.at[which], raw_r.at[2, which, c], ep=next_plane * per + col)

    def next_send(which):
        loop(chunks, lambda c: next_copy(which, c, cols_of(c)).start())

    next_block = pl.ds(pl.multiple_of((next_plane * per - first) * cap, 16), rows_g)
    own_block = pl.ds(pl.multiple_of((z * per - first) * cap, 16), rows_g)
    block = pl.ds(0, rows_g)

    def near_send(which):
        shares[which].wait()

        def place(c):
            near[which, :, cols_of(c)] = dot(pn[...], tx[which, :, cols_of(c)], NN).astype(BF16)

        loop(chunks, place)

        def send(k):
            j = lax.rem(col + 1 + k, per)

            @pl.when(j != col)
            def _():
                near_copy(which, j).start()

            @pl.when(j == col)
            def _():
                local(near.at[which, rows(mine)], xd.at[which, t, rows(me)], r_sem.at[which, me]).start()

        loop(per, send)

    near_send(0)
    next_send(0)
    near_send(1)

    for load in loads:
        load.start()

    def source_of(q):
        return jnp.where(q == 0, far_outer, jnp.where(q == 1, far_inner, next_plane)) * per + col

    def cross_copy(q, which, c, at):
        return remote(fwd.at[q, which, next_block, at], raw.at[q, which, block, at],
                      f_sem.at[q, which, col], raw_r.at[q, which, c], ep=own_outer * per + col)

    def spread_copy(src_rows, q, which, j, at):
        src = source_of(q)
        return remote(src_rows, xd.at[which, t, rows(src), at],
                      f_sem.at[q, which, j], r_sem.at[which, src], ep=z * per + j)

    def spread(buf, base, q, which, at):
        src = source_of(q)

        def one(k):
            j = lax.rem(col + 1 + k, per)
            src_rows = buf.at[q, which, rows(base + j), at]

            @pl.when(j != col)
            def _():
                spread_copy(src_rows, q, which, j, at).start()

            @pl.when(j == col)
            def _():
                local(src_rows, xd.at[which, t, rows(src), at], r_sem.at[which, src]).start()

        loop(per, one)

    def scatter(q, begin, count):
        def step(k):
            i = begin + k
            which = i // chunks
            c = i % chunks
            at = cols_of(c)
            part = raw.at[q, which, block, at]
            remote(part, part, raw_s.at[0, 0], raw_r.at[q, which, c], ep=my_relay).wait_recv()
            spread(raw, 0, q, which, at)

        loop(count, step)

    def relay_start(q):
        remote(tg, rt.at[q], meta_s.at[0], meta_r.at[q], ep=my_relay).wait_recv()
        pq[q] = placing(rt[q, 0:1, :], rt[q, 1:2, :])

    def relay(q, begin, count):
        def step(k):
            i = begin + k
            which = i // chunks
            c = i % chunks
            at = cols_of(c)
            remote(raw.at[q, which, :, at], raw.at[q, which, :, at], raw_s.at[0, 0],
                   raw_r.at[q, which, c], ep=my_relay).wait_recv()

            @pl.when((q == 0) & (i == 2 * chunks - 2))
            def _():
                raw_send()

            fwd[q, which, :, at] = dot(pq[q], raw[q, which, :, at], NN).astype(BF16)

            cross_copy(q, which, c, at).start()
            spread(fwd, own_inner * per - first, q, which, at)

        loop(count, step)

    def pair_copy(which, s):
        block = xd.at[which, t, rows(s)]
        return remote(block, block, ps_sem.at[which, s], pr_sem.at[which, s], tp=other)

    def arrive(g):
        for which in range(2):
            def pass_on(j, which=which):
                s = g * per + j
                local(near.at[which, rows(0)], xd.at[which, t, rows(s)], r_sem.at[which, s]).wait()
                pair_copy(which, s).start()

            loop(per, pass_on)
        for which in range(2):
            def joined(j, which=which):
                s = g * per + j
                block = xd.at[which, other, rows(s)]
                remote(block, block, ps_sem.at[which, s], pr_sem.at[which, s], tp=other).wait_recv()

            loop(per, joined)

    def lane_sums(v):
        ones = jnp.ones((8, v.shape[1]), BF16)
        high = v.astype(BF16)
        low = (v - high.astype(F32)).astype(BF16)
        return dot(ones, high, NT) + dot(ones, low, NT)

    def exchange(i, c):
        at = cols_of(c)
        return remote(give.at[i % 2, :, at], got.at[i % 2, :, at], xs_sem.at[i, c],
                      xr_sem.at[i, c], tp=other)

    def gate_exchange(g):
        grp = pl.ds(g * per, per)
        return remote(gp.at[grp], gpp.at[grp], qs_sem.at[g], qr_sem.at[g], tp=other)

    def back_slot(g):
        far_slot = jnp.where(g == far_outer, 0, 1)
        return jnp.where(g == z, 2, jnp.where(g == next_plane, 3, far_slot))

    def back_copy(s, c, at):
        slot = back_slot(s // per)
        return remote(rg.at[rows(s), at], back.at[slot, rows(mine), at], bs_sem.at[s],
                      br_sem.at[slot, c], ep=z * per + s % per)

    def gathered(slot, c, at, sem):
        local(near.at[0, block, at], back.at[slot, block, at], sem.at[slot, c]).wait()

    def up_copy(slot, c, at):
        to = jnp.where(slot == 3, 2, slot)
        return remote(back.at[slot, own_block, at], back.at[to, own_block, at],
                      bf_sem.at[slot], bg_sem.at[to, c], ep=own_inner * per + col)

    def up(slot):
        def step(c):
            at = cols_of(c)
            gathered(slot, c, at, br_sem)
            up_copy(slot, c, at).start()

        loop(chunks, step)

    def gate_back(s):
        return remote(gt.at[s, first_row], gback.at[me, first_row], hs_sem.at[s], hr_sem.at[me], ep=s)

    def rows_out(g, c):
        at = cols_of(c)
        slot = back_slot(g)

        def out(j):
            s = g * per + lax.rem(col + 1 + j, per)

            @pl.when(j == per - 1)
            def _():
                local(rg.at[rows(s), at], back.at[slot, rows(mine), at], br_sem.at[slot, c]).start()

            @pl.when(j != per - 1)
            def _():
                back_copy(s, c, at).start()

        loop(per, out)

    def group(i, g):
        arrive(g)
        r = pl.ds(pl.multiple_of(g * rows_g, 16), rows_g)
        pg[...] = dot(xd[0, 0, r, :], wg[0], NN) + dot(xd[0, 1, r, :], wg[1], NN)
        pu[...] = dot(xd[0, 0, r, :], wu[0], NN) + dot(xd[0, 1, r, :], wu[1], NN)

        def gates_in(j):
            s = g * per + j
            local(gs.at[0, first_row], gr.at[s, first_row], gr_sem.at[s]).wait()
            column = jnp.transpose(jnp.broadcast_to(gr[s, 0:1, :], (8, 128)))
            gcol[rows(j), :] = jnp.broadcast_to(column[:cap, 0:1], (cap, 128))

        loop(per, gates_in)
        dh = dot(xd[1, 0, r, :], wd[:, :share], NT) + dot(xd[1, 1, r, :], wd[:, share:], NT)
        a = pg[...]
        b = pu[...]
        gate = gcol[:, 0:1]
        sig = jax.nn.sigmoid(a)
        silu = a * sig
        hidden = (silu * b).astype(BF16).astype(F32)
        prod[...] = hidden * dh
        scaled = gate * dh
        gpgu[r, :units] = (scaled * b * sig * (1.0 + a * (1.0 - sig))).astype(BF16)
        gpgu[r, units:] = (scaled * silu).astype(BF16)
        wt[r, :] = (gate * hidden).astype(BF16)

        def part(c):
            at = cols_of(c)

            @pl.when(i > 1)
            def _():
                exchange(i - 2, c).wait_send()

            def half_rows_of(side):
                return (
                    dot(gpgu[r, :units], wg[side, at, :], NT)
                    + dot(gpgu[r, units:], wu[side, at, :], NT)
                ).astype(BF16)

            give[i % 2, :, at] = half_rows_of(other)
            rg[r, at] = half_rows_of(t)
            exchange(i, c).start()

        def gate_sum(j):
            gp[g * per + j, :, :cap] = lane_sums(prod[rows(j), :])

        def finish(c):
            at = cols_of(c)
            exchange(i, c).wait_recv()
            rg[r, at] = (rg[r, at].astype(F32) + got[i % 2, :, at].astype(F32)).astype(BF16)

            rows_out(g, c)

        loop(per, gate_sum)
        gate_exchange(g).start()

        def gates_out(j):
            s = g * per + j
            gt[s] = gp[s] + gpp[s]

            @pl.when(s == me)
            def _():
                local(gt.at[s, first_row], gback.at[me, first_row], hr_sem.at[me]).start()

            @pl.when(s != me)
            def _():
                gate_back(s).start()

        def column(c):
            @pl.when(c < chunks)
            def _():
                part(c)

            @pl.when(c == 1)
            def _():
                gate_exchange(g).wait_recv()
                loop(per, gates_out)

            @pl.when(c > 0)
            def _():
                finish(c - 1)

        loop(chunks + 1, column)

    def comb_copy(q, at, c):
        there = far_inner * per + col
        if q == 0:
            return remote(comb.at[0, :, at], mid.at[:, at], cs_sem.at[0, c], mr_sem.at[c], ep=there)
        return remote(comb.at[1, :, at], far.at[:, at], cs_sem.at[1, c], cr_sem.at[c], ep=there)

    def combine(q, c):
        at = cols_of(c)
        gathered(q, c, at, br_sem)
        gathered(q, c, at, bg_sem)
        comb[q, :, at] = dot(pq[q], back[q, :, at], TN).astype(BF16)
        comb_copy(q, at, c).start()

    def merge_copy(at, c):
        return remote(tx.at[1, :, at], far.at[:, at], ms_sem.at[c], cr_sem.at[c],
                      ep=own_outer * per + col)

    def merge(c):
        at = cols_of(c)
        gathered(3, c, at, br_sem)
        close = dot(pm[...], back[3, own_block, at], TN)
        local(far.at[:, at], mid.at[:, at], mr_sem.at[c]).wait()
        tx[1, :, at] = (close + mid[:, at].astype(F32)).astype(BF16)
        merge_copy(at, c).start()

    gp[...] = jnp.zeros_like(gp)
    for load in loads:
        load.wait()

    def phase(i):
        @pl.when(inner & (i % 2 == 0))
        def _():
            relay_start(i // 2)

        @pl.when(inner & (i < planes - 1))
        def _():
            relay(i // 2, jnp.where(i == 1, chunks, 0), jnp.where(i == 2, 2 * chunks, chunks))

        @pl.when(inner & (i == 1))
        def _():
            next_send(1)

        @pl.when((outer & (i > 0)) | (i > 1))
        def _():
            scatter(
                jnp.where(inner, 2, jnp.where(i == 1, 0, 1)),
                jnp.where(i == 3, chunks, 0),
                jnp.where(i == 1, 2 * chunks, chunks),
            )

        @pl.when(inner & (i == 2))
        def _():
            loop(chunks, lambda c: combine(0, c))

        @pl.when(outer & (i == 3))
        def _():
            up(3)

        on_inner = jnp.where(i == 1, far_outer, jnp.where(i == 2, far_inner, own_outer))
        on_outer = jnp.where(i == 1, far_outer, jnp.where(i == 2, own_inner, far_inner))
        group(i, jnp.where(i == 0, z, jnp.where(inner, on_inner, on_outer)))

        @pl.when(outer & (i % 2 == 1))
        def _():
            up(i // 2)

        @pl.when(outer & (i == 1))
        def _():
            next_send(1)

        @pl.when(outer & (i < 2))
        def _():
            scatter(2, i * chunks, chunks)

    loop(planes, phase)

    acc[...] = jnp.zeros_like(acc)

    @pl.when(inner)
    def _():
        remote(tg, rt.at[2], meta_s.at[1], meta_r.at[2], ep=my_relay).wait_recv()
        plane_rows = lax.broadcasted_iota(jnp.int32, (rows_g, toks), 0) + z * rows_g
        plane_rows = plane_rows.astype(F32)
        pm[...] = jnp.where(
            (plane_rows == rt[2, 0:1, :]) | (plane_rows == rt[2, 1:2, :]), 1.0, 0.0
        ).astype(BF16)

    def grads(i):
        side = i // chunks
        at = cols_of(i % chunks)
        wide = cols_of(i)
        q = dot(xd[0, side, :, at], gpgu[...], TN).astype(BF16)
        wg[side, at, :] = q[:, :units]
        wu[side, at, :] = q[:, units:]
        f = q.astype(F32)
        f = f * f
        sqs[0, :, wide] = lane_sums(f[:, :units])
        sqs[1, :, wide] = lane_sums(f[:, units:])
        d = dot(wt[...], xd[1, side, :, at], TN).astype(BF16)
        wd[:, wide] = d
        d = d.astype(F32)
        acc[...] += lane_sums(d * d)

        @pl.when(inner & (i % 2 == 0))
        def _():
            merge(i // 2)

        @pl.when(inner & (i % 2 == 1))
        def _():
            combine(1, i // 2)

    loop(2 * chunks, grads)

    stores = [
        local(a, b, o_sem.at[i])
        for i, (a, b) in enumerate(((wg, ggw), (wu, guw), (wd, gdw)))
    ]
    for store in stores:
        store.start()
    squares = remote(sqs, sqr, e_sem.at[0], e_sem.at[1], tp=other)
    squares.start()
    sqd[...] = acc[0:1, :] / (2 * share)
    squares.wait()
    sqg[...] = (sqs[0, 0:1, :] + sqr[0, 0:1, :]) / full_units
    squ[...] = (sqs[1, 0:1, :] + sqr[1, 0:1, :]) / full_units

    loop(n, lambda e: local(gt.at[e, first_row], gback.at[e, first_row], hr_sem.at[e]).wait())
    slots = lax.broadcasted_iota(jnp.int32, (cap, toks), 0)

    def look_up(e, carry):
        column = jnp.transpose(jnp.broadcast_to(gback[e, 0:1, :], (8, 128)))[:cap, 0:1]
        at = (slots + e * cap).astype(F32)
        return tuple(
            v + jnp.where(at == tg[k:k + 1, :], column, 0.0) for k, v in enumerate(carry)
        )

    zero = jnp.zeros((cap, toks), F32)
    found = lax.fori_loop(0, n, look_up, (zero, zero))
    for k in range(2):
        ggate[k:k + 1, :] = jnp.sum(found[k], axis=0, keepdims=True)

    meta.wait_send()
    for which in range(2):
        loop(chunks, lambda c, which=which: raw_copy(which, c).wait_send())

    @pl.when(outer)
    def _():
        close_meta.wait_send()
        for slot in (0, 1, 3):
            up_copy(slot, 0, pl.ds(0, share)).wait_send()

    for which in range(2):
        next_copy(which, 0, pl.ds(0, share)).wait_send()

    def drain_near(j):
        @pl.when(j != col)
        def _():
            for which in range(2):
                near_copy(which, j).wait_send()

    loop(per, drain_near)

    def drain_spread(j):
        for q in range(3):
            for which in range(2):
                @pl.when(j != col)
                def _(q=q, which=which):
                    spread_copy(raw.at[q, which, rows(j)], q, which, j, pl.ds(0, share)).wait_send()

                if q < 2:
                    @pl.when(inner & (j == col))
                    def _(q=q, which=which):
                        cross_copy(q, which, 0, pl.ds(0, share)).wait_send()

    loop(per, drain_spread)

    def drain(k):
        d = peer(k)
        gate_copy(d).wait_send()
        gate_back(d).wait_send()

    loop(n - 1, drain)

    def drain_rows(s):
        for which in range(2):
            pair_copy(which, s).wait_send()

        @pl.when(s % per != col)
        def _():
            back_copy(s, 0, pl.ds(0, share)).wait_send()

    loop(n, drain_rows)

    def drain_group(g):
        gate_exchange(g).wait_send()

        @pl.when(g >= planes - 2)
        def _():
            loop(chunks, lambda c: exchange(g, c).wait_send())

    loop(planes, drain_group)

    def last(c):
        at = cols_of(c)

        def finish_rows(part):
            gathered(2, c, at, br_sem)
            close = dot(pn[part, :], back[2, part, at], TN)
            local(far.at[:, at], far.at[:, at], cr_sem.at[c]).wait()
            tx[0, :, at] = (close + far[:, at].astype(F32)).astype(BF16)

        @pl.when(inner)
        def _():
            gathered(2, c, at, bg_sem)
            finish_rows(pl.ds(0, hr))

        @pl.when(outer)
        def _():
            finish_rows(own_block)

        local(tx.at[0, :, at], gtok.at[:, at], go_sem.at[c]).start()

    loop(chunks, last)

    @pl.when(inner)
    def _():
        for q in range(2):
            loop(chunks, lambda c, q=q: comb_copy(q, cols_of(c), c).wait_send())
        loop(chunks, lambda c: merge_copy(cols_of(c), c).wait_send())

    for store in stores:
        store.wait()
    loop(chunks, lambda c: local(tx.at[0, :, cols_of(c)], gtok.at[:, cols_of(c)], go_sem.at[c]).wait())


def relay_scratch(n, planes, cap, units, share, tile, toks):
    total = n * cap
    group = total // planes
    hr = n // 2 * cap
    chunks = share // tile
    half = n // 2
    per = n // planes
    width = 2 * share
    arrays = [
        ((2, 2, total, share), BF16), ((2, toks, share), BF16), ((hr, toks), BF16),
        ((2, hr, share), BF16), ((8, toks), F32), ((3, 8, toks), F32), ((2, hr, toks), BF16),
        ((3, 2, toks, share), BF16), ((2, 2, hr, share), BF16),
        ((2, share, units), BF16), ((2, share, units), BF16), ((units, width), BF16),
        ((n, 8, 128), F32), ((n, 8, 128), F32), ((group, 128), F32),
        ((group, units), F32), ((group, units), F32), ((group, units), F32),
        ((total, 2 * units), BF16), ((total, units), BF16),
        ((2, group, share), BF16), ((2, group, share), BF16), ((total, share), BF16),
        ((n, 8, 128), F32), ((n, 8, 128), F32), ((n, 8, 128), F32), ((n, 8, 128), F32),
        ((4, hr, share), BF16), ((2, toks, share), BF16), ((toks, share), BF16),
        ((toks, share), BF16), ((group, toks), BF16), ((2, 8, width), F32), ((2, 8, width), F32), ((8, units), F32),
    ]
    sems = [
        (3,), (2,), (2, chunks), (3, 2, chunks), (2,), (3,), (2, per), (2, n), (3, 2, per),
        (n,), (n,), (2, n), (2, n), (planes, chunks), (planes, chunks), (planes,), (planes,),
        (n,), (4, chunks), (2, chunks), (chunks,), (n,), (n,), (3,), (2,), (chunks,),
        (2,), (chunks,), (chunks,), (4,), (3, chunks),
    ]
    size = 0
    for dims, kind in arrays:
        count = jnp.dtype(kind).itemsize
        for d in dims:
            count *= d
        size += count
    return arrays, sems, size


def fused_relay(n, planes, cap, toks, tile, tokens, cotangent, gates, experts, w_gate, w_up, w_down):
    width, units = w_gate.shape
    cores = lax.axis_size("tp")
    share = width // cores
    any_spec = pl.BlockSpec(memory_space=pl.ANY)
    vmem = pl.BlockSpec(memory_space=pltpu.VMEM)
    shape = jax.ShapeDtypeStruct
    arrays, sems, _ = relay_scratch(n, planes, cap, units, share, tile, toks)
    return pl.pallas_call(
        functools.partial(relay_kernel, n, planes, cap, units, share, tile, toks, units * cores),
        out_shape=(
            shape((toks, share), BF16),
            shape((2, toks), F32),
            shape((2, share, units), BF16),
            shape((2, share, units), BF16),
            shape((units, width), BF16),
            shape((1, width), F32),
            shape((1, width), F32),
            shape((1, units), F32),
        ),
        in_specs=[any_spec, any_spec, vmem, vmem, any_spec, any_spec, any_spec],
        out_specs=(any_spec, vmem, any_spec, any_spec, any_spec, vmem, vmem, vmem),
        scratch_shapes=[pltpu.VMEM(dims, kind) for dims, kind in arrays]
        + [pltpu.SemaphoreType.DMA(dims) for dims in sems],
        compiler_params=pltpu.CompilerParams(
            collective_id=0, has_side_effects=True, vmem_limit_bytes=VMEM_BYTES
        ),
    )(tokens, cotangent, gates.T, experts.T,
      w_gate.reshape(2, share, units), w_up.reshape(2, share, units), w_down)


def body(tokens, cotangent, gates, experts, gate_w, up_w, down_w):
    tok_rows, width = tokens.shape
    top_count = experts.shape[1]
    n_ep = lax.axis_size("ep")
    n_cores = lax.axis_size("tp")
    capacity = 3 * tok_rows * top_count // (2 * n_ep)
    cap = -(-capacity // 16) * 16
    n_slots = n_ep * cap
    share = width // n_cores
    tile = 512
    units = gate_w.shape[2]
    _, _, size = relay_scratch(n_ep, PLANES, cap, units, share, tile, tok_rows)
    if n_ep % PLANES == 0 and tok_rows < n_ep // 2 * cap and size + (1 << 20) < VMEM_BYTES:
        gtok, ggate, ggw, guw, gdw, sqg, squ, sqd = fused_relay(
            n_ep, PLANES, cap, tok_rows, tile, tokens, cotangent, gates, experts,
            gate_w[0], up_w[0], down_w[0],
        )
        return (
            gtok, ggate.T, ggw.reshape(gate_w.shape), guw.reshape(up_w.shape), gdw[None],
            sqg, squ, sqd,
        )
    flat_ids = experts.reshape(-1)
    onehot = (flat_ids[:, None] == jnp.arange(n_ep, dtype=jnp.int32)[None, :]).astype(jnp.int32)
    earlier = jnp.cumsum(onehot, axis=0) - onehot
    slot_of = jnp.sum(earlier * onehot, axis=1)
    target = flat_ids * cap + slot_of
    placing = (target[None, :] == jnp.arange(n_slots, dtype=jnp.int32)[:, None]).astype(F32)
    place_tok = jnp.sum(placing.reshape(n_slots, tok_rows, top_count), axis=2).astype(BF16)
    send_gate = jnp.dot(placing, gates.reshape(-1), precision=lax.Precision.HIGHEST)
    send_gate = jnp.pad(send_gate.reshape(n_ep, 1, cap), ((0, 0), (0, 7), (0, 128 - cap)))
    share = width // n_cores
    offset = lax.axis_index("tp") * share
    tok_share = lax.dynamic_slice_in_dim(tokens, offset, share, 1)
    cot_share = lax.dynamic_slice_in_dim(cotangent, offset, share, 1)
    send_x = jnp.dot(place_tok, tok_share, preferred_element_type=F32).astype(BF16)
    send_dy = jnp.dot(place_tok, cot_share, preferred_element_type=F32).astype(BF16)
    back, gback, ggw, guw, gdw, sq, sqd = fused(
        n_ep, cap, send_x.reshape(n_ep, cap, share), send_dy.reshape(n_ep, cap, share),
        send_gate, gate_w[0], up_w[0], down_w[0],
    )
    grad_tokens = lax.dot_general(
        place_tok, back.reshape(n_slots, share), TN, preferred_element_type=F32
    ).astype(BF16)
    grad_gates = jnp.dot(
        gback[:, 0, :cap].reshape(n_slots), placing, precision=lax.Precision.HIGHEST
    ).reshape(tok_rows, top_count)
    full_units = gate_w.shape[2] * n_cores
    sq = sq[:, :, :, 0, :].reshape(2, width) / full_units
    return (
        grad_tokens,
        grad_gates,
        ggw.reshape(gate_w.shape),
        guw.reshape(up_w.shape),
        gdw[None],
        sq[0][None],
        sq[1][None],
        sqd[0:1] / width,
    )


def solution(mesh):
    placed = (
        P("ep", None),
        P("ep", None),
        P("ep", None),
        P("ep", None),
        P("ep", None, "tp"),
        P("ep", None, "tp"),
        P("ep", "tp", None),
    )
    return jax.shard_map(
        body,
        mesh=mesh,
        in_specs=placed,
        out_specs=(
            P("ep", "tp"),
            P("ep", None),
            P("ep", None, "tp"),
            P("ep", None, "tp"),
            P("ep", "tp", None),
            P("ep", None),
            P("ep", None),
            P("ep", "tp"),
        ),
        check_vma=False,
    )
```

```python
import functools

import jax
import jax.numpy as jnp
from jax import lax
from jax.experimental import pallas as pl
from jax.experimental.pallas import tpu as pltpu
from jax.sharding import PartitionSpec as P

MESH = pl.DeviceIdType.MESH
BF16 = jnp.bfloat16
F32 = jnp.float32
NN = (((1,), (0,)), ((), ()))
NT = (((1,), (1,)), ((), ()))
TN = (((0,), (0,)), ((), ()))
VMEM_BYTES = 67043328
PLANES = 4


def dot(a, b, dims, precision=None):
    return lax.dot_general(a, b, dims, precision=precision, preferred_element_type=F32)


def kernel(
    n, cap, units, share, groups, tile,
    sx, sdy, sg, wg_in, wu_in, wd_in,
    back, gback, ggw, guw, gdw, sq_out, sqd_out,
    xr, dyr, gr, wg, wu, wd, pg, pu, prod, gpgu, wt, keep, give, got, rg,
    gp, gpp, gt, gcol, sqs, sqr, acc,
    w_sem, s_sem, r_sem, gs_sem, gr_sem, fs_sem, fr_sem,
    ps_sem, pr_sem, qs_sem, qr_sem, bs_sem, br_sem, hs_sem, hr_sem, o_sem, e_sem,
):
    me = lax.axis_index("ep")
    t = lax.axis_index("tp")
    other = lax.axis_size("tp") - 1 - t
    per = n // groups
    rows_g = per * cap

    def rows(s):
        return pl.ds(pl.multiple_of(s * cap, 16), cap)

    def remote(src, dst, send, recv, **where):
        return pltpu.make_async_remote_copy(
            src_ref=src, dst_ref=dst, send_sem=send, recv_sem=recv,
            device_id=where, device_id_type=MESH,
        )

    def loop(count, fn):
        def step(i, carry):
            fn(i)
            return carry
        lax.fori_loop(0, count, step, 0)

    def peer(k):
        return lax.rem(me + n // 2 + k + jnp.where(k >= n - n // 2, 1, 0), n)

    barrier = pltpu.get_barrier_semaphore()
    loop(n - 1, lambda k: pl.semaphore_signal(
        barrier, inc=1, device_id={"ep": peer(k)}, device_id_type=MESH))
    pl.semaphore_signal(barrier, inc=1, device_id={"tp": other}, device_id_type=MESH)
    pl.semaphore_wait(barrier, n)

    ins = ((sx, xr), (sdy, dyr))
    for which, (src, dst) in enumerate(ins):
        def send(k, which=which, src=src, dst=dst):
            d = peer(k)
            remote(src.at[d], dst.at[t, rows(me)], s_sem.at[which, d],
                   r_sem.at[which, me], ep=d).start()
        loop(n - 1, send)
        pltpu.make_async_copy(src.at[me], dst.at[t, rows(me)], r_sem.at[which, me]).start()
        if which == 0:
            def send_gate(k):
                d = peer(k)
                remote(sg.at[d], gr.at[me], gs_sem.at[d], gr_sem.at[me], ep=d).start()
            loop(n - 1, send_gate)
            pltpu.make_async_copy(sg.at[me], gr.at[me], gr_sem.at[me]).start()
            loads = [
                pltpu.make_async_copy(a, b, w_sem.at[i])
                for i, (a, b) in enumerate(((wg_in, wg), (wu_in, wu), (wd_in, wd)))
            ]
            for load in loads:
                load.start()

    def order(i):
        return lax.rem(me // per + groups // 2 + i, groups)

    def arrive(which, g):
        src, dst = ins[which]

        def pass_on(j):
            s = g * per + j
            pltpu.make_async_copy(src.at[0], dst.at[t, rows(s)], r_sem.at[which, s]).wait()
            remote(dst.at[t, rows(s)], dst.at[t, rows(s)], fs_sem.at[which, s],
                   fr_sem.at[which, s], tp=other).start()

        def joined(j):
            s = g * per + j
            remote(dst.at[other, rows(s)], dst.at[other, rows(s)], fs_sem.at[which, s],
                   fr_sem.at[which, s], tp=other).wait_recv()

        loop(per, pass_on)
        loop(per, joined)

    def span(g):
        return pl.ds(pl.multiple_of(g * rows_g, 16), rows_g)

    for load in loads:
        load.wait()

    def forward(i):
        g = order(i)
        arrive(0, g)
        r = span(g)
        pg[r, :] = dot(xr[0, r, :], wg[0], NN) + dot(xr[1, r, :], wg[1], NN)
        pu[r, :] = dot(xr[0, r, :], wu[0], NN) + dot(xr[1, r, :], wu[1], NN)

    loop(groups, forward)

    def exchange(g):
        r = span(g)
        grp = pl.ds(g * per, per)
        return (
            remote(give.at[r], got.at[r], ps_sem.at[g], pr_sem.at[g], tp=other),
            remote(gp.at[grp], gpp.at[grp], qs_sem.at[g], qr_sem.at[g], tp=other),
        )

    def back_copies(s):
        return (
            remote(rg.at[rows(s)], back.at[me], bs_sem.at[s], br_sem.at[me], ep=s),
            remote(gt.at[s], gback.at[me], hs_sem.at[s], hr_sem.at[me], ep=s),
        )

    def finish(g):
        for copy in exchange(g):
            copy.wait_recv()

        def one(j):
            s = g * per + j
            r = rows(s)
            rg[r, :] = (keep[r, :].astype(F32) + got[r, :].astype(F32)).astype(BF16)
            gt[s] = gp[s] + gpp[s]

        loop(per, one)

        def out(j):
            s = g * per + j

            @pl.when(s == me)
            def _():
                pltpu.make_async_copy(rg.at[rows(s)], back.at[me], br_sem.at[me]).start()
                pltpu.make_async_copy(gt.at[s], gback.at[me], hr_sem.at[me]).start()

            @pl.when(s != me)
            def _():
                for copy in back_copies(s):
                    copy.start()

        loop(per, out)

    ones_units = jnp.ones((8, units), F32)

    def backward(i):
        g = order(i)
        arrive(1, g)

        def gates_in(j):
            s = g * per + j
            pltpu.make_async_copy(sg.at[0], gr.at[s], gr_sem.at[s]).wait()
            column = jnp.transpose(gr[s])
            gcol[rows(s), :] = jnp.broadcast_to(column[:cap, 0:1], (cap, 128))

        loop(per, gates_in)
        r = span(g)
        dh = dot(dyr[0, r, :], wd[:, :share], NT) + dot(dyr[1, r, :], wd[:, share:], NT)
        a = pg[r, :]
        b = pu[r, :]
        gate = gcol[r, 0:1]
        sig = jax.nn.sigmoid(a)
        silu = a * sig
        hidden = (silu * b).astype(BF16).astype(F32)
        prod[...] = hidden * dh
        scaled = gate * dh
        gpg = (scaled * b * sig * (1.0 + a * (1.0 - sig))).astype(BF16)
        gpu = (scaled * silu).astype(BF16)
        gpgu[r, :units] = gpg
        gpgu[r, units:] = gpu
        wt[r, :] = (gate * hidden).astype(BF16)

        def part(c):
            cols = pl.ds(pl.multiple_of(c * tile, tile), tile)
            for half, dst in ((other, give), (t, keep)):
                dst[r, cols] = (
                    dot(gpgu[r, :units], wg[half, cols, :], NT)
                    + dot(gpgu[r, units:], wu[half, cols, :], NT)
                ).astype(BF16)

        loop(share // tile, part)

        def gate_sum(j):
            p = prod[pl.ds(pl.multiple_of(j * cap, 16), cap), :]
            gp[g * per + j, :, :cap] = dot(ones_units, p, NT, lax.Precision.HIGHEST)

        loop(per, gate_sum)
        for copy in exchange(g):
            copy.start()

        @pl.when(i > 0)
        def _():
            finish(order(i - 1 + groups))

    gp[...] = jnp.zeros_like(gp)
    loop(groups, backward)
    finish(order(groups - 1))

    acc[...] = jnp.zeros_like(acc)
    for h in range(2):
        def grads(c, h=h):
            cols = pl.ds(pl.multiple_of(c * tile, tile), tile)
            q = dot(xr[h, :, cols], gpgu[...], TN).astype(BF16)
            wg[h, cols, :] = q[:, :units]
            wu[h, cols, :] = q[:, units:]
            f = q.astype(F32)
            f = f * f
            sqs[0, h, c] = dot(ones_units, f[:, :units], NT, lax.Precision.HIGHEST)
            sqs[1, h, c] = dot(ones_units, f[:, units:], NT, lax.Precision.HIGHEST)
            d = dot(wt[...], dyr[h, :, cols], TN).astype(BF16)
            wd[:, pl.ds(pl.multiple_of(h * share + c * tile, tile), tile)] = d
            d = d.astype(F32)
            acc[...] += d * d

        loop(share // tile, grads)

    stores = [
        pltpu.make_async_copy(a, b, o_sem.at[i])
        for i, (a, b) in enumerate(((wg, ggw), (wu, guw), (wd, gdw)))
    ]
    for store in stores:
        store.start()
    squares = remote(sqs, sqr, e_sem.at[0], e_sem.at[1], tp=other)
    squares.start()
    sqd_out[...] = dot(jnp.ones((8, tile), F32), acc[...], NT, lax.Precision.HIGHEST)
    squares.wait()
    sq_out[...] = sqs[...] + sqr[...]
    for store in stores:
        store.wait()

    def drain(k):
        d = peer(k)
        for which, (src, dst) in enumerate(ins):
            remote(src.at[d], dst.at[t, rows(me)], s_sem.at[which, d],
                   r_sem.at[which, me], ep=d).wait_send()
        remote(sg.at[d], gr.at[me], gs_sem.at[d], gr_sem.at[me], ep=d).wait_send()
        for copy in back_copies(d):
            copy.wait_send()

    loop(n - 1, drain)

    def drain_pair(s):
        for which, (src, dst) in enumerate(ins):
            remote(dst.at[t, rows(s)], dst.at[t, rows(s)], fs_sem.at[which, s],
                   fr_sem.at[which, s], tp=other).wait_send()
        pltpu.make_async_copy(rg.at[rows(s)], back.at[s], br_sem.at[s]).wait()
        pltpu.make_async_copy(gt.at[s], gback.at[s], hr_sem.at[s]).wait()

    loop(n, drain_pair)

    def drain_group(g):
        for copy in exchange(g):
            copy.wait_send()

    loop(groups, drain_group)


def fused(n, cap, send_x, send_dy, send_gate, w_gate, w_up, w_down):
    width, units = w_gate.shape
    share = send_x.shape[2]
    total = n * cap
    groups = 4
    tile = 512
    any_spec = pl.BlockSpec(memory_space=pl.ANY)
    vmem = pl.BlockSpec(memory_space=pltpu.VMEM)
    sq_shape = (2, 2, share // tile, 8, tile)
    dma = pltpu.SemaphoreType.DMA
    shape = jax.ShapeDtypeStruct
    return pl.pallas_call(
        functools.partial(kernel, n, cap, units, share, groups, tile),
        out_shape=(
            shape((n, cap, share), BF16),
            shape((n, 8, 128), F32),
            shape((2, share, units), BF16),
            shape((2, share, units), BF16),
            shape((units, width), BF16),
            shape(sq_shape, F32),
            shape((8, units), F32),
        ),
        in_specs=[any_spec] * 6,
        out_specs=(any_spec,) * 5 + (vmem, vmem),
        scratch_shapes=[
            pltpu.VMEM((2, total, share), BF16),
            pltpu.VMEM((2, total, share), BF16),
            pltpu.VMEM((n, 8, 128), F32),
            pltpu.VMEM((2, share, units), BF16),
            pltpu.VMEM((2, share, units), BF16),
            pltpu.VMEM((units, width), BF16),
            pltpu.VMEM((total, units), F32),
            pltpu.VMEM((total, units), F32),
            pltpu.VMEM((total // groups, units), F32),
            pltpu.VMEM((total, 2 * units), BF16),
            pltpu.VMEM((total, units), BF16),
            pltpu.VMEM((total, share), BF16),
            pltpu.VMEM((total, share), BF16),
            pltpu.VMEM((total, share), BF16),
            pltpu.VMEM((total, share), BF16),
            pltpu.VMEM((n, 8, 128), F32),
            pltpu.VMEM((n, 8, 128), F32),
            pltpu.VMEM((n, 8, 128), F32),
            pltpu.VMEM((total, 128), F32),
            pltpu.VMEM(sq_shape, F32),
            pltpu.VMEM(sq_shape, F32),
            pltpu.VMEM((units, tile), F32),
            dma((3,)), dma((2, n)), dma((2, n)), dma((n,)), dma((n,)), dma((2, n)), dma((2, n)),
            dma((groups,)), dma((groups,)), dma((groups,)), dma((groups,)),
            dma((n,)), dma((n,)), dma((n,)), dma((n,)), dma((3,)), dma((2,)),
        ],
        compiler_params=pltpu.CompilerParams(
            collective_id=0, has_side_effects=True, vmem_limit_bytes=63 << 20
        ),
    )(send_x, send_dy, send_gate,
      w_gate.reshape(2, share, units), w_up.reshape(2, share, units), w_down)


def relay_kernel(
    n, planes, cap, units, share, tile, toks, full_units,
    tok, cot, gates, experts, wg_in, wu_in, wd_in,
    gtok, ggate_out, ggw, guw, gdw, sqg_out, squ_out, sqd_out,
    xd, tx, pn, near, tg, rt, pq, raw, fwd, wg, wu, wd, gs, gr, gcol, pg, pu, prod, gpgu, wt,
    give, got, rg, gp, gpp, gt, gback, back, comb, far, mid, pm, sqs, sqr, acc, ggate, sqg, squ, sqd,
    w_sem, t_sem, raw_s, raw_r, meta_s, meta_r, s_sem, r_sem, f_sem, gs_sem, gr_sem, ps_sem, pr_sem,
    xs_sem, xr_sem, qs_sem, qr_sem, bs_sem, br_sem, cs_sem, cr_sem, hs_sem, hr_sem, o_sem, e_sem, go_sem,
    n_sem, ms_sem, mr_sem, bf_sem, small_sem,
):
    me = lax.axis_index("ep")
    t = lax.axis_index("tp")
    other = lax.axis_size("tp") - 1 - t
    per = n // planes
    half = n // 2
    rows_g = per * cap
    hr = half * cap
    chunks = share // tile
    z = me // per
    col = me % per
    h = z // (planes // 2)
    oh = 1 - h
    first = h * half
    mine = me - first
    own_inner, own_outer = 1 + h, (planes - 1) * h
    far_inner, far_outer = 1 + oh, (planes - 1) * oh
    inner = z == own_inner
    outer = z == own_outer
    next_plane = own_inner + own_outer - z
    my_relay = far_inner * per + col
    my_q = jnp.where(inner, 1, 0)

    def rows(s):
        return pl.ds(pl.multiple_of(s * cap, 16), cap)

    def cols_of(c):
        return pl.ds(pl.multiple_of(c * tile, tile), tile)

    def remote(src, dst, send, recv, **where):
        return pltpu.make_async_remote_copy(
            src_ref=src, dst_ref=dst, send_sem=send, recv_sem=recv,
            device_id=where, device_id_type=MESH,
        )

    def local(src, dst, sem):
        return pltpu.make_async_copy(src, dst, sem)

    def loop(count, fn):
        def step(i, carry):
            fn(i)
            return carry
        lax.fori_loop(0, count, step, 0)

    def peer(k):
        return lax.rem(me + n // 2 + k + jnp.where(k >= n - n // 2, 1, 0), n)

    barrier = pltpu.get_barrier_semaphore()
    loop(n - 1, lambda k: pl.semaphore_signal(
        barrier, inc=1, device_id={"ep": peer(k)}, device_id_type=MESH))
    pl.semaphore_signal(barrier, inc=1, device_id={"tp": other}, device_id_type=MESH)

    my_cols = pl.ds(pl.multiple_of(t * share, share), share)
    ins = (tok, cot)
    shares = [local(a.at[:, my_cols], tx.at[w], t_sem.at[w]) for w, a in enumerate(ins)]
    loads = [
        local(a, b, w_sem.at[i])
        for i, (a, b) in enumerate(((wg_in, wg), (wu_in, wu), (wd_in, wd)))
    ]
    for copy in shares:
        copy.start()

    e0, e1 = experts[0:1, :], experts[1:2, :]
    which_expert = lax.broadcasted_iota(jnp.int32, (n, toks), 0)
    hit0 = (which_expert == e0).astype(F32)
    hit1 = (which_expert == e1).astype(F32)
    before = (
        lax.broadcasted_iota(jnp.int32, (toks, toks), 0)
        < lax.broadcasted_iota(jnp.int32, (toks, toks), 1)
    ).astype(F32).astype(BF16)
    earlier = dot((hit0 + hit1).astype(BF16), before, NN)
    t0 = e0.astype(F32) * cap + jnp.sum(earlier * hit0, axis=0, keepdims=True)
    t1 = e1.astype(F32) * cap + jnp.sum(earlier * hit1, axis=0, keepdims=True)
    tg[0:1, :] = t0
    tg[1:2, :] = t1
    tg[2:4, :] = gates[...]
    tg[4:8, :] = jnp.zeros((4, toks), F32)

    half_rows = (lax.broadcasted_iota(jnp.int32, (hr, toks), 0) + first * cap).astype(F32)

    def placing(a, b):
        return jnp.where((half_rows == a) | (half_rows == b), 1.0, 0.0).astype(BF16)

    pn[...] = placing(t0, t1)

    columns = jnp.transpose(tg[...])
    c0, c1, g0, g1 = (columns[:, i:i + 1] for i in range(4))
    lanes = lax.broadcasted_iota(jnp.int32, (toks, 128), 1)
    lanes = jnp.where(lanes < cap, lanes, -2 * n * cap).astype(F32)

    def gate_row(e):
        base = (e * cap).astype(F32)
        picked = jnp.where(c0 - base == lanes, g0, 0.0) + jnp.where(c1 - base == lanes, g1, 0.0)
        gs[e, 0:1, :] = jnp.sum(picked, axis=0, keepdims=True)

    loop(n, gate_row)

    pl.semaphore_wait(barrier, n)

    def raw_copy(which, c):
        at = pl.ds(pl.multiple_of(t * share + c * tile, tile), tile)
        return remote(ins[which].at[:, at], raw.at[my_q, which, :, cols_of(c)],
                      raw_s.at[which, c], raw_r.at[my_q, which, c], ep=my_relay)

    def raw_send():
        for which in range(2):
            loop(chunks, lambda c, which=which: raw_copy(which, c).start())

    first_row = pl.ds(0, 1)

    def gate_copy(d):
        return remote(gs.at[d, first_row], gr.at[me, first_row], gs_sem.at[d], gr_sem.at[me], ep=d)

    loop(n - 1, lambda k: gate_copy(peer(k)).start())
    local(gs.at[me, first_row], gr.at[me, first_row], gr_sem.at[me]).start()

    meta = remote(tg, rt.at[my_q], meta_s.at[0], meta_r.at[my_q], ep=my_relay)
    meta.start()
    close_meta = remote(tg, rt.at[2], meta_s.at[1], meta_r.at[2], ep=own_inner * per + col)

    @pl.when(outer)
    def _():
        close_meta.start()

    @pl.when(outer)
    def _():
        raw_send()

    def near_copy(which, j):
        return remote(near.at[which, rows(z * per - first + j)], xd.at[which, t, rows(me)],
                      s_sem.at[which, j], r_sem.at[which, me], ep=z * per + j)

    def next_copy(which, c, at):
        return remote(near.at[which, next_block, at], raw.at[2, which, block, at],
                      n_sem.at[which], raw_r.at[2, which, c], ep=next_plane * per + col)

    def next_send(which):
        loop(chunks, lambda c: next_copy(which, c, cols_of(c)).start())

    next_block = pl.ds(pl.multiple_of((next_plane * per - first) * cap, 16), rows_g)
    own_block = pl.ds(pl.multiple_of((z * per - first) * cap, 16), rows_g)
    block = pl.ds(0, rows_g)

    def near_send(which):
        shares[which].wait()

        def place(c):
            near[which, :, cols_of(c)] = dot(pn[...], tx[which, :, cols_of(c)], NN).astype(BF16)

        loop(chunks, place)

        def send(k):
            j = lax.rem(col + 1 + k, per)

            @pl.when(j != col)
            def _():
                near_copy(which, j).start()

            @pl.when(j == col)
            def _():
                local(near.at[which, rows(mine)], xd.at[which, t, rows(me)], r_sem.at[which, me]).start()

        loop(per, send)

    near_send(0)
    next_send(0)
    near_send(1)
    next_send(1)

    for load in loads:
        load.start()

    def source_of(q):
        return jnp.where(q == 0, far_outer, jnp.where(q == 1, far_inner, next_plane)) * per + col

    def cross_copy(q, which, c, at):
        return remote(fwd.at[q, which, next_block, at], raw.at[q, which, block, at],
                      f_sem.at[q, which, col], raw_r.at[q, which, c], ep=own_outer * per + col)

    def spread_copy(src_rows, q, which, j, at):
        src = source_of(q)
        return remote(src_rows, xd.at[which, t, rows(src), at],
                      f_sem.at[q, which, j], r_sem.at[which, src], ep=z * per + j)

    def spread(buf, base, q, which, at):
        src = source_of(q)

        def one(k):
            j = lax.rem(col + 1 + k, per)
            src_rows = buf.at[q, which, rows(base + j), at]

            @pl.when(j != col)
            def _():
                spread_copy(src_rows, q, which, j, at).start()

            @pl.when(j == col)
            def _():
                local(src_rows, xd.at[which, t, rows(src), at], r_sem.at[which, src]).start()

        loop(per, one)

    def scatter(q, begin, count):
        def step(k):
            i = begin + k
            which = i // chunks
            c = i % chunks
            at = cols_of(c)
            part = raw.at[q, which, block, at]
            remote(part, part, raw_s.at[0, 0], raw_r.at[q, which, c], ep=my_relay).wait_recv()
            spread(raw, 0, q, which, at)

        loop(count, step)

    def relay_start(q):
        remote(tg, rt.at[q], meta_s.at[0], meta_r.at[q], ep=my_relay).wait_recv()
        pq[q] = placing(rt[q, 0:1, :], rt[q, 1:2, :])

    def relay(q, begin, count):
        def step(k):
            i = begin + k
            which = i // chunks
            c = i % chunks
            at = cols_of(c)
            remote(raw.at[q, which, :, at], raw.at[q, which, :, at], raw_s.at[0, 0],
                   raw_r.at[q, which, c], ep=my_relay).wait_recv()

            @pl.when((q == 0) & (i == 2 * chunks - 2))
            def _():
                raw_send()

            fwd[q, which, :, at] = dot(pq[q], raw[q, which, :, at], NN).astype(BF16)

            cross_copy(q, which, c, at).start()
            spread(fwd, own_inner * per - first, q, which, at)

        loop(count, step)

    def pair_copy(which, s):
        block = xd.at[which, t, rows(s)]
        return remote(block, block, ps_sem.at[which, s], pr_sem.at[which, s], tp=other)

    def arrive(g):
        for which in range(2):
            def pass_on(j, which=which):
                s = g * per + j
                local(near.at[which, rows(0)], xd.at[which, t, rows(s)], r_sem.at[which, s]).wait()
                pair_copy(which, s).start()

            loop(per, pass_on)
        for which in range(2):
            def joined(j, which=which):
                s = g * per + j
                block = xd.at[which, other, rows(s)]
                remote(block, block, ps_sem.at[which, s], pr_sem.at[which, s], tp=other).wait_recv()

            loop(per, joined)

    def lane_sums(v):
        ones = jnp.ones((8, v.shape[1]), BF16)
        high = v.astype(BF16)
        low = (v - high.astype(F32)).astype(BF16)
        return dot(ones, high, NT) + dot(ones, low, NT)

    def exchange(i, c):
        at = cols_of(c)
        return remote(give.at[i % 2, :, at], got.at[i % 2, :, at], xs_sem.at[i, c],
                      xr_sem.at[i, c], tp=other)

    def gate_exchange(g):
        grp = pl.ds(g * per, per)
        return remote(gp.at[grp], gpp.at[grp], qs_sem.at[g], qr_sem.at[g], tp=other)

    def back_slot(g):
        far_slot = jnp.where(g == far_outer, 0, 1)
        return jnp.where(g == z, 2, jnp.where(g == next_plane, 3, far_slot))

    def back_copy(s, c, at):
        slot = back_slot(s // per)
        plane = jnp.where(straight(s // per), own_inner, z)
        return remote(rg.at[rows(s), at], back.at[slot, rows(mine), at], bs_sem.at[s],
                      br_sem.at[back_mark(s // per), c], ep=plane * per + s % per)

    def straight(g):
        return outer & (g == far_inner)

    def back_mark(g):
        return jnp.where(straight(g), 5, back_slot(g))

    def gathered(mark, c, at):
        local(near.at[0, block, at], back.at[0, block, at], br_sem.at[mark, c]).wait()

    def up_copy(slot, c, at):
        to = jnp.where(slot == 3, 2, slot)
        return remote(back.at[slot, own_block, at], back.at[to, own_block, at],
                      bf_sem.at[slot], br_sem.at[4 + to, c], ep=own_inner * per + col)

    def up(slot):
        def step(c):
            at = cols_of(c)
            gathered(slot, c, at)
            up_copy(slot, c, at).start()

        loop(chunks, step)

    def gate_back(s):
        return remote(gt.at[s, first_row], gback.at[me, first_row], hs_sem.at[s], hr_sem.at[me], ep=s)

    def rows_out(g, c):
        at = cols_of(c)
        slot = back_slot(g)

        def out(j):
            s = g * per + lax.rem(col + 1 + j, per)

            @pl.when((j == per - 1) & jnp.logical_not(straight(g)))
            def _():
                local(rg.at[rows(s), at], back.at[slot, rows(mine), at], br_sem.at[slot, c]).start()

            @pl.when((j != per - 1) | straight(g))
            def _():
                back_copy(s, c, at).start()

        loop(per, out)

    def group(i, g):
        arrive(g)
        r = pl.ds(pl.multiple_of(g * rows_g, 16), rows_g)
        pg[...] = dot(xd[0, 0, r, :], wg[0], NN) + dot(xd[0, 1, r, :], wg[1], NN)
        pu[...] = dot(xd[0, 0, r, :], wu[0], NN) + dot(xd[0, 1, r, :], wu[1], NN)

        def gates_in(j):
            s = g * per + j
            local(gs.at[0, first_row], gr.at[s, first_row], gr_sem.at[s]).wait()
            column = jnp.transpose(jnp.broadcast_to(gr[s, 0:1, :], (8, 128)))
            gcol[rows(j), :] = jnp.broadcast_to(column[:cap, 0:1], (cap, 128))

        loop(per, gates_in)
        dh = dot(xd[1, 0, r, :], wd[:, :share], NT) + dot(xd[1, 1, r, :], wd[:, share:], NT)
        a = pg[...]
        b = pu[...]
        gate = gcol[:, 0:1]
        sig = jax.nn.sigmoid(a)
        silu = a * sig
        hidden = (silu * b).astype(BF16).astype(F32)
        prod[...] = hidden * dh
        scaled = gate * dh
        gpgu[r, :units] = (scaled * b * sig * (1.0 + a * (1.0 - sig))).astype(BF16)
        gpgu[r, units:] = (scaled * silu).astype(BF16)
        wt[r, :] = (gate * hidden).astype(BF16)

        def part(c):
            at = cols_of(c)

            @pl.when(i > 1)
            def _():
                exchange(i - 2, c).wait_send()

            def half_rows_of(side):
                return (
                    dot(gpgu[r, :units], wg[side, at, :], NT)
                    + dot(gpgu[r, units:], wu[side, at, :], NT)
                ).astype(BF16)

            give[i % 2, :, at] = half_rows_of(other)
            rg[r, at] = half_rows_of(t)
            exchange(i, c).start()

        def gate_sum(j):
            gp[g * per + j, :, :cap] = lane_sums(prod[rows(j), :])

        def finish(c):
            at = cols_of(c)
            exchange(i, c).wait_recv()
            rg[r, at] = (rg[r, at].astype(F32) + got[i % 2, :, at].astype(F32)).astype(BF16)

            rows_out(g, c)

        loop(per, gate_sum)
        gate_exchange(g).start()

        def gates_out(j):
            s = g * per + j
            gt[s] = gp[s] + gpp[s]

            @pl.when(s == me)
            def _():
                local(gt.at[s, first_row], gback.at[me, first_row], hr_sem.at[me]).start()

            @pl.when(s != me)
            def _():
                gate_back(s).start()

        def column(c):
            @pl.when(c < chunks)
            def _():
                part(c)

            @pl.when(c == 1)
            def _():
                gate_exchange(g).wait_recv()
                loop(per, gates_out)

            @pl.when(c > 0)
            def _():
                finish(c - 1)

        loop(chunks + 1, column)

    def comb_copy(q, at, c):
        there = far_inner * per + col
        if q == 0:
            return remote(comb.at[0, :, at], mid.at[:, at], cs_sem.at[0, c], mr_sem.at[c], ep=there)
        return remote(comb.at[1, :, at], far.at[:, at], cs_sem.at[1, c], cr_sem.at[c], ep=there)

    def combine(q, c):
        at = cols_of(c)
        gathered(q, c, at)
        gathered(4 + q, c, at)
        comb[q, :, at] = dot(pq[q], back[q, :, at], TN).astype(BF16)
        comb_copy(q, at, c).start()

    def merge_copy(at, c):
        return remote(tx.at[1, :, at], far.at[:, at], ms_sem.at[c], cr_sem.at[c],
                      ep=own_outer * per + col)

    def merge(c):
        at = cols_of(c)
        gathered(3, c, at)
        close = dot(pm[...], back[3, own_block, at], TN)
        local(far.at[:, at], mid.at[:, at], mr_sem.at[c]).wait()
        tx[1, :, at] = (close + mid[:, at].astype(F32)).astype(BF16)
        merge_copy(at, c).start()

    gp[...] = jnp.zeros_like(gp)
    for load in loads:
        load.wait()

    def phase(i):
        @pl.when(inner & (i % 2 == 0))
        def _():
            relay_start(i // 2)
            relay(i // 2, 0, chunks)

        @pl.when((inner & (i == 2)) | (outer & (i == 0)))
        def _():
            scatter(2, 0, chunks)

        @pl.when(inner & ((i == 1) | (i == 2)))
        def _():
            relay(i - 1, chunks, chunks)

        @pl.when((inner & (i == 2)) | (outer & (i == 1)))
        def _():
            scatter(2, chunks, chunks)

        @pl.when(outer & (i > 0))
        def _():
            scatter(jnp.where(i == 3, 1, 0), jnp.where(i == 1, 0, chunks), chunks)

        on_inner = jnp.where(i == 1, far_outer, jnp.where(i == 2, far_inner, own_outer))
        on_outer = jnp.where(i == 1, own_inner, jnp.where(i == 2, far_outer, far_inner))
        group(i, jnp.where(i == 0, z, jnp.where(inner, on_inner, on_outer)))

        @pl.when(inner & (i == 2))
        def _():
            loop(chunks, lambda c: combine(0, c))

        @pl.when(outer & (i == 2))
        def _():
            scatter(1, 0, chunks)

        @pl.when(outer & (i == 2))
        def _():
            up(0)
            up(3)

    loop(planes, phase)

    acc[...] = jnp.zeros_like(acc)

    @pl.when(inner)
    def _():
        remote(tg, rt.at[2], meta_s.at[1], meta_r.at[2], ep=my_relay).wait_recv()
        plane_rows = lax.broadcasted_iota(jnp.int32, (rows_g, toks), 0) + z * rows_g
        plane_rows = plane_rows.astype(F32)
        pm[...] = jnp.where(
            (plane_rows == rt[2, 0:1, :]) | (plane_rows == rt[2, 1:2, :]), 1.0, 0.0
        ).astype(BF16)

    def grads(i):
        side = i // chunks
        at = cols_of(i % chunks)
        wide = cols_of(i)
        q = dot(xd[0, side, :, at], gpgu[...], TN).astype(BF16)
        wg[side, at, :] = q[:, :units]
        wu[side, at, :] = q[:, units:]
        f = q.astype(F32)
        f = f * f
        sqs[0, :, wide] = lane_sums(f[:, :units])
        sqs[1, :, wide] = lane_sums(f[:, units:])
        d = dot(wt[...], xd[1, side, :, at], TN).astype(BF16)
        wd[:, wide] = d
        d = d.astype(F32)
        acc[...] += lane_sums(d * d)

        @pl.when(inner & (i % 2 == 0))
        def _():
            merge(i // 2)

        @pl.when(inner & (i % 2 == 1))
        def _():
            combine(1, i // 2)

    loop(2 * chunks, grads)

    stores = [
        local(a, b, o_sem.at[i])
        for i, (a, b) in enumerate(((wg, ggw), (wu, guw), (wd, gdw)))
    ]
    for store in stores:
        store.start()
    squares = remote(sqs, sqr, e_sem.at[0], e_sem.at[1], tp=other)
    squares.start()
    sqd[...] = acc[0:1, :] / (2 * share)
    squares.wait()
    sqg[...] = (sqs[0, 0:1, :] + sqr[0, 0:1, :]) / full_units
    squ[...] = (sqs[1, 0:1, :] + sqr[1, 0:1, :]) / full_units
    small = [
        local(a, b, small_sem.at[i])
        for i, (a, b) in enumerate(
            ((sqg, sqg_out), (squ, squ_out), (sqd, sqd_out), (ggate, ggate_out))
        )
    ]
    for copy in small[:3]:
        copy.start()

    loop(n, lambda e: local(gt.at[e, first_row], gback.at[e, first_row], hr_sem.at[e]).wait())
    slots = lax.broadcasted_iota(jnp.int32, (cap, toks), 0)

    def look_up(e, carry):
        column = jnp.transpose(jnp.broadcast_to(gback[e, 0:1, :], (8, 128)))[:cap, 0:1]
        at = (slots + e * cap).astype(F32)
        return tuple(
            v + jnp.where(at == tg[k:k + 1, :], column, 0.0) for k, v in enumerate(carry)
        )

    zero = jnp.zeros((cap, toks), F32)
    found = lax.fori_loop(0, n, look_up, (zero, zero))
    for k in range(2):
        ggate[k:k + 1, :] = jnp.sum(found[k], axis=0, keepdims=True)
    small[3].start()

    meta.wait_send()
    for which in range(2):
        loop(chunks, lambda c, which=which: raw_copy(which, c).wait_send())

    @pl.when(outer)
    def _():
        close_meta.wait_send()
        for slot in (0, 3):
            up_copy(slot, 0, pl.ds(0, share)).wait_send()

    for which in range(2):
        next_copy(which, 0, pl.ds(0, share)).wait_send()

    def drain_near(j):
        @pl.when(j != col)
        def _():
            for which in range(2):
                near_copy(which, j).wait_send()

    loop(per, drain_near)

    def drain_spread(j):
        for q in range(3):
            for which in range(2):
                @pl.when(j != col)
                def _(q=q, which=which):
                    spread_copy(raw.at[q, which, rows(j)], q, which, j, pl.ds(0, share)).wait_send()

                if q < 2:
                    @pl.when(inner & (j == col))
                    def _(q=q, which=which):
                        cross_copy(q, which, 0, pl.ds(0, share)).wait_send()

    loop(per, drain_spread)

    def drain(k):
        d = peer(k)
        gate_copy(d).wait_send()
        gate_back(d).wait_send()

    loop(n - 1, drain)

    def drain_rows(s):
        for which in range(2):
            pair_copy(which, s).wait_send()

        @pl.when((s % per != col) | straight(s // per))
        def _():
            back_copy(s, 0, pl.ds(0, share)).wait_send()

    loop(n, drain_rows)

    def drain_group(g):
        gate_exchange(g).wait_send()

        @pl.when(g >= planes - 2)
        def _():
            loop(chunks, lambda c: exchange(g, c).wait_send())

    loop(planes, drain_group)

    def last(c):
        at = cols_of(c)

        def finish_rows(part):
            gathered(2, c, at)
            close = dot(pn[part, :], back[2, part, at], TN)
            local(far.at[:, at], far.at[:, at], cr_sem.at[c]).wait()
            tx[0, :, at] = (close + far[:, at].astype(F32)).astype(BF16)

        @pl.when(inner)
        def _():
            gathered(6, c, at)
            finish_rows(pl.ds(0, hr))

        @pl.when(outer)
        def _():
            finish_rows(own_block)

        local(tx.at[0, :, at], gtok.at[:, at], go_sem.at[c]).start()

    loop(chunks, last)

    @pl.when(inner)
    def _():
        for q in range(2):
            loop(chunks, lambda c, q=q: comb_copy(q, cols_of(c), c).wait_send())
        loop(chunks, lambda c: merge_copy(cols_of(c), c).wait_send())

    for copy in small:
        copy.wait()
    for store in stores:
        store.wait()
    loop(chunks, lambda c: local(tx.at[0, :, cols_of(c)], gtok.at[:, cols_of(c)], go_sem.at[c]).wait())


def relay_scratch(n, planes, cap, units, share, tile, toks):
    total = n * cap
    group = total // planes
    hr = n // 2 * cap
    chunks = share // tile
    half = n // 2
    per = n // planes
    width = 2 * share
    arrays = [
        ((2, 2, total, share), BF16), ((2, toks, share), BF16), ((hr, toks), BF16),
        ((2, hr, share), BF16), ((8, toks), F32), ((3, 8, toks), F32), ((2, hr, toks), BF16),
        ((3, 2, toks, share), BF16), ((2, 2, hr, share), BF16),
        ((2, share, units), BF16), ((2, share, units), BF16), ((units, width), BF16),
        ((n, 8, 128), F32), ((n, 8, 128), F32), ((group, 128), F32),
        ((group, units), F32), ((group, units), F32), ((group, units), F32),
        ((total, 2 * units), BF16), ((total, units), BF16),
        ((2, group, share), BF16), ((2, group, share), BF16), ((total, share), BF16),
        ((n, 8, 128), F32), ((n, 8, 128), F32), ((n, 8, 128), F32), ((n, 8, 128), F32),
        ((4, hr, share), BF16), ((2, toks, share), BF16), ((toks, share), BF16),
        ((toks, share), BF16), ((group, toks), BF16), ((2, 8, width), F32), ((2, 8, width), F32), ((8, units), F32),
        ((2, toks), F32), ((1, width), F32), ((1, width), F32), ((1, units), F32),
    ]
    sems = [
        (3,), (2,), (2, chunks), (3, 2, chunks), (2,), (3,), (2, per), (2, n), (3, 2, per),
        (n,), (n,), (2, n), (2, n), (planes, chunks), (planes, chunks), (planes,), (planes,),
        (n,), (7, chunks), (2, chunks), (chunks,), (n,), (n,), (3,), (2,), (chunks,),
        (2,), (chunks,), (chunks,), (4,), (4,),
    ]
    size = 0
    for dims, kind in arrays:
        count = jnp.dtype(kind).itemsize
        for d in dims:
            count *= d
        size += count
    return arrays, sems, size


def fused_relay(n, planes, cap, toks, tile, tokens, cotangent, gates, experts, w_gate, w_up, w_down):
    width, units = w_gate.shape
    cores = lax.axis_size("tp")
    share = width // cores
    any_spec = pl.BlockSpec(memory_space=pl.ANY)
    vmem = pl.BlockSpec(memory_space=pltpu.VMEM)
    shape = jax.ShapeDtypeStruct
    arrays, sems, _ = relay_scratch(n, planes, cap, units, share, tile, toks)
    return pl.pallas_call(
        functools.partial(relay_kernel, n, planes, cap, units, share, tile, toks, units * cores),
        out_shape=(
            shape((toks, share), BF16),
            shape((2, toks), F32),
            shape((2, share, units), BF16),
            shape((2, share, units), BF16),
            shape((units, width), BF16),
            shape((1, width), F32),
            shape((1, width), F32),
            shape((1, units), F32),
        ),
        in_specs=[any_spec, any_spec, vmem, vmem, any_spec, any_spec, any_spec],
        out_specs=(any_spec,) * 8,
        scratch_shapes=[pltpu.VMEM(dims, kind) for dims, kind in arrays]
        + [pltpu.SemaphoreType.DMA(dims) for dims in sems],
        compiler_params=pltpu.CompilerParams(
            collective_id=0, has_side_effects=True, vmem_limit_bytes=VMEM_BYTES
        ),
    )(tokens, cotangent, gates.T, experts.T,
      w_gate.reshape(2, share, units), w_up.reshape(2, share, units), w_down)


def body(tokens, cotangent, gates, experts, gate_w, up_w, down_w):
    tok_rows, width = tokens.shape
    top_count = experts.shape[1]
    n_ep = lax.axis_size("ep")
    n_cores = lax.axis_size("tp")
    capacity = 3 * tok_rows * top_count // (2 * n_ep)
    cap = -(-capacity // 16) * 16
    n_slots = n_ep * cap
    share = width // n_cores
    tile = 512
    units = gate_w.shape[2]
    _, _, size = relay_scratch(n_ep, PLANES, cap, units, share, tile, tok_rows)
    if n_ep % PLANES == 0 and tok_rows < n_ep // 2 * cap and size + (1 << 20) < VMEM_BYTES:
        gtok, ggate, ggw, guw, gdw, sqg, squ, sqd = fused_relay(
            n_ep, PLANES, cap, tok_rows, tile, tokens, cotangent, gates, experts,
            gate_w[0], up_w[0], down_w[0],
        )
        return (
            gtok, ggate.T, ggw.reshape(gate_w.shape), guw.reshape(up_w.shape), gdw[None],
            sqg, squ, sqd,
        )
    flat_ids = experts.reshape(-1)
    onehot = (flat_ids[:, None] == jnp.arange(n_ep, dtype=jnp.int32)[None, :]).astype(jnp.int32)
    earlier = jnp.cumsum(onehot, axis=0) - onehot
    slot_of = jnp.sum(earlier * onehot, axis=1)
    target = flat_ids * cap + slot_of
    placing = (target[None, :] == jnp.arange(n_slots, dtype=jnp.int32)[:, None]).astype(F32)
    place_tok = jnp.sum(placing.reshape(n_slots, tok_rows, top_count), axis=2).astype(BF16)
    send_gate = jnp.dot(placing, gates.reshape(-1), precision=lax.Precision.HIGHEST)
    send_gate = jnp.pad(send_gate.reshape(n_ep, 1, cap), ((0, 0), (0, 7), (0, 128 - cap)))
    share = width // n_cores
    offset = lax.axis_index("tp") * share
    tok_share = lax.dynamic_slice_in_dim(tokens, offset, share, 1)
    cot_share = lax.dynamic_slice_in_dim(cotangent, offset, share, 1)
    send_x = jnp.dot(place_tok, tok_share, preferred_element_type=F32).astype(BF16)
    send_dy = jnp.dot(place_tok, cot_share, preferred_element_type=F32).astype(BF16)
    back, gback, ggw, guw, gdw, sq, sqd = fused(
        n_ep, cap, send_x.reshape(n_ep, cap, share), send_dy.reshape(n_ep, cap, share),
        send_gate, gate_w[0], up_w[0], down_w[0],
    )
    grad_tokens = lax.dot_general(
        place_tok, back.reshape(n_slots, share), TN, preferred_element_type=F32
    ).astype(BF16)
    grad_gates = jnp.dot(
        gback[:, 0, :cap].reshape(n_slots), placing, precision=lax.Precision.HIGHEST
    ).reshape(tok_rows, top_count)
    full_units = gate_w.shape[2] * n_cores
    sq = sq[:, :, :, 0, :].reshape(2, width) / full_units
    return (
        grad_tokens,
        grad_gates,
        ggw.reshape(gate_w.shape),
        guw.reshape(up_w.shape),
        gdw[None],
        sq[0][None],
        sq[1][None],
        sqd[0:1] / width,
    )


def solution(mesh):
    placed = (
        P("ep", None),
        P("ep", None),
        P("ep", None),
        P("ep", None),
        P("ep", None, "tp"),
        P("ep", None, "tp"),
        P("ep", "tp", None),
    )
    return jax.shard_map(
        body,
        mesh=mesh,
        in_specs=placed,
        out_specs=(
            P("ep", "tp"),
            P("ep", None),
            P("ep", None, "tp"),
            P("ep", None, "tp"),
            P("ep", "tp", None),
            P("ep", None),
            P("ep", None),
            P("ep", "tp"),
        ),
        check_vma=False,
    )
```
